256 devices in a mesh: sp: 16 (over y, x), tp: 16 (over z, core).
Axes of the slice: x: 4, y: 4, z: 8, core: 2. Of those that a mesh axis runs over, the one named last changes fastest.
Arguments:
- residual: bfloat16 [6144, 2048], P(('sp', 'tp')), may hold values from -40 to 40
- queries: bfloat16 [6144, 16, 256], P('sp', 'tp'), may hold values from -8.8 to 8.8
- query_rope: bfloat16 [6144, 16, 64], P('sp', 'tp'), may hold values from -72 to 72
- latent: bfloat16 [6144, 512], P('sp'), may hold values from -320 to 320
- key_rope: bfloat16 [6144, 32], P('sp'), may hold values from -48 to 48
- latent_gain: float32 [512], replicated, may hold values from 0.1 to 1.9
- key_weight: bfloat16 [512, 16, 256], P(None, 'tp'), may hold values from -0.25 to 0.25
- value_weight: bfloat16 [512, 16, 256], P(None, 'tp'), may hold values from -0.25 to 0.25
- out_weight: bfloat16 [16, 256, 2048], P('tp'), may hold values from -0.09375 to 0.09375
- norm_gain: float32 [2048], replicated, may hold values from 0.1 to 1.9
- routes: int32 [6144, 2], P('sp'), may hold values from 0 to 31, as said below
- group_gate: float32 [6144], P(('sp', 'tp')), may hold values from 0.5 to 1
- expert_share: float32 [6144, 2], P(('sp', 'tp')), may hold values from 0.2 to 1
- gate_weight: bfloat16 [32, 2048, 4096], P('sp', None, 'tp'), may hold values from -0.125 to 0.125
- up_weight: bfloat16 [32, 2048, 4096], P('sp', None, 'tp'), may hold values from -0.125 to 0.125
- down_weight: bfloat16 [32, 4096, 2048], P('sp', 'tp'), may hold values from -0.1875 to 0.1875
Outputs:
- layer_out: bfloat16 [6144, 2048], P(('sp', 'tp'))
The draws below stay inside these ranges and needn't reach their ends.
Inputs may be any that keep to these rules, and one draw needn't show every extreme that they name: `routes`: each token names two different experts of one group; expert e belongs to group e // 8. In each aligned block of 24 tokens no expert is named more than 2 times, and one expert, the same in every block, is named exactly 2 times in every block.
All inputs are finite; a program needn't handle non-finite values.
Results may differ from the reference program's by a relative error of at most 0.025.
Values may be sent and summed in bfloat16 or wider, within the bound.
A program may use at most 64 MiB of HBM per device.

```python
import math
import jax
import jax.numpy as jnp
from jax import lax

D = 2048
PAIRS = 16
DK_A = 64
DV_A = 64
DK_B = 192
DV_B = 192
DR = 32
LATENT = 512
FF = 4096
GROUPS = 4
TOPK = 2
SEQ = 6144
PAIR_DEV = 1
ROWS = 24
FF_DEV = 256
EXPERTS = 32
CAP = 2
N_TP = 16


def rough_field(key, salt_value, columns):
    values = jnp.clip(jax.random.normal(jax.random.fold_in(key, salt_value), (SEQ, columns), jnp.float32), -4.0, 4.0)
    return values


def draw_residual(key, part):
    return (0.25 * rough_field(key, 40, D)).astype(jnp.bfloat16)


def draw_latent(key, part):
    return rough_field(key, 50, LATENT).astype(jnp.bfloat16)


def draw_queries(key, part):
    own_key = jax.random.fold_in(key, 23)
    array_shape = (SEQ, PAIRS, DK_A + DK_B)
    return jnp.clip(2.2 * jax.random.normal(own_key, array_shape, jnp.float32), -8.75, 8.75).astype(jnp.bfloat16)


def draw_query_rope(key, part):
    own_key = jax.random.fold_in(key, 21)
    array_shape = (SEQ, PAIRS, 2 * DR)
    return jnp.clip(2.2 * jax.random.normal(own_key, array_shape, jnp.float32), -8.75, 8.75).astype(jnp.bfloat16)


def draw_key_rope(key, part):
    own_key = jax.random.fold_in(key, 22)
    base_values = jnp.clip(jax.random.normal(own_key, (SEQ, DR), jnp.float32), -4.0, 4.0)
    return base_values.astype(jnp.bfloat16)


def draw_routes(key, part):
    blocks = SEQ // ROWS
    within = EXPERTS // GROUPS
    pair_total = EXPERTS // 2
    hot_rows = 0
    while hot_rows + (ROWS - hot_rows + pair_total - 1) // pair_total != CAP:
        hot_rows += 1
    key_list = jax.random.split(jax.random.fold_in(key, 31), 5)
    favored = jax.random.randint(key_list[0], (), 0, EXPERTS, dtype=jnp.int32)
    favored_group = favored // within
    favored_place = favored % within
    member = jnp.arange(within, dtype=jnp.int32)
    ranking = jax.random.randint(key_list[1], (blocks, GROUPS, within), 0, 1 << 20, dtype=jnp.int32) * within + member
    place_order = jnp.argsort(ranking, axis=2).astype(jnp.int32)
    leading = place_order[:, :, :1]
    swapped = jnp.where(place_order == favored_place, leading, place_order)
    swapped = jnp.where(member[None, None, :] == 0, favored_place, swapped)
    is_favored = (jnp.arange(GROUPS, dtype=jnp.int32) == favored_group)[None, :, None]
    place_order = jnp.where(is_favored, swapped, place_order)
    expert_table = place_order + (jnp.arange(GROUPS, dtype=jnp.int32) * within)[None, :, None]
    pair_table = expert_table.reshape(blocks, pair_total, 2)
    pair_ids = jnp.arange(pair_total, dtype=jnp.int32)
    pair_rank = jax.random.randint(key_list[2], (blocks, pair_total), 0, 1 << 20, dtype=jnp.int32) * pair_total + pair_ids
    pair_rank = jnp.where(pair_ids[None, :] == favored_group * (within // 2), -1, pair_rank)
    pair_order = jnp.argsort(pair_rank, axis=1)
    pair_table = jnp.take_along_axis(pair_table, pair_order[:, :, None], axis=1)
    row_ids = jnp.arange(ROWS, dtype=jnp.int32)
    cycled = jnp.take(pair_table, (row_ids - hot_rows) % pair_total, axis=1)
    favored_row = jnp.take(expert_table, favored_group, axis=1)
    partner = jnp.take(favored_row, 1 + row_ids % (within - 1), axis=1)
    hot_pair = jnp.stack([jnp.broadcast_to(favored, partner.shape), partner], axis=2)
    chosen = jnp.where((row_ids < hot_rows)[None, :, None], hot_pair, cycled)
    flip_bits = jax.random.randint(key_list[3], (blocks, ROWS, 1), 0, 2, dtype=jnp.int32)
    chosen = jnp.where(flip_bits == 1, chosen[:, :, ::-1], chosen)
    shuffle = jnp.argsort(jax.random.randint(key_list[4], (blocks, ROWS), 0, 1 << 20, dtype=jnp.int32) * ROWS + row_ids[None, :], axis=1)
    chosen = jnp.take_along_axis(chosen, shuffle[:, :, None], axis=1)
    return chosen.reshape(SEQ, 2).astype(jnp.int32)


def block_levels(rng, shape, pieces, smallest, top_value):
    def one(axis_at, parts):
        steps = jax.random.uniform(jax.random.fold_in(jax.random.fold_in(rng, 6), axis_at), (parts,), jnp.float32, smallest / len(pieces), top_value / len(pieces))
        return jnp.repeat(jnp.exp(steps), shape[axis_at] // parts).reshape((-1,) + (1,) * (len(shape) - axis_at - 1))

    level = one(*pieces[0])
    for cut in pieces[1:]:
        level = level * one(*cut)
    return level


def scatter_about(key, shape, deviation, limit, cuts=(), kind=jnp.bfloat16):
    array = jax.random.normal(key, shape, jnp.float32) * deviation
    if len(cuts) > 0:
        array = block_levels(key, shape, cuts, -0.22, 0.18) * array
    return jnp.clip(array, min=-limit, max=limit).astype(kind)


def setup_inputs(seed: int = 0) -> dict:
    splits = jax.random.split(jax.random.key(seed), 17)
    residual = draw_residual(jax.random.fold_in(splits[16], 71), 0)
    queries = draw_queries(jax.random.fold_in(splits[16], 71), 0)
    query_rope = draw_query_rope(jax.random.fold_in(splits[16], 71), 0)
    latent = draw_latent(jax.random.fold_in(splits[16], 71), 0)
    key_rope = draw_key_rope(jax.random.fold_in(splits[16], 71), 0)
    latent_gain = jnp.clip(1.0 + 0.18 * jax.random.normal(splits[5], (LATENT,), jnp.float32), 0.1, 1.9)
    key_weight = scatter_about(splits[6], (LATENT, PAIRS, DK_A + DK_B), LATENT ** -0.5, 0.25, ((1, 16),))
    value_weight = scatter_about(splits[7], (LATENT, PAIRS, DV_A + DV_B), LATENT ** -0.5, 0.25, ((1, 16),))
    out_weight = scatter_about(splits[8], (PAIRS, DV_A + DV_B, D), (PAIRS * (DV_A + DV_B)) ** -0.5, 0.09375, ((0, 16),))
    norm_gain = jnp.clip(1.0 + 0.18 * jax.random.normal(splits[9], (D,), jnp.float32), 0.1, 1.9)
    routes = draw_routes(jax.random.fold_in(splits[16], 71), 0)
    group_gate = jnp.clip(jnp.exp(math.log(1.0) - 0.6931472 * jax.random.uniform(splits[11], (SEQ,), jnp.float32) ** block_levels(splits[11], (SEQ,), ((0, 256),), -0.2, 0.2)), 0.5, 1.0)
    expert_share = jnp.clip(jnp.exp(math.log(1.0) - 1.609438 * jax.random.uniform(splits[12], (SEQ, TOPK), jnp.float32) ** block_levels(splits[12], (SEQ, TOPK), ((0, 256),), -0.2, 0.2)), 0.2, 1.0)
    gate_weight = scatter_about(splits[13], (EXPERTS, D, FF), D ** -0.5, 0.125, ((0, 16), (2, 16)))
    up_weight = scatter_about(splits[14], (EXPERTS, D, FF), D ** -0.5, 0.125, ((0, 16), (2, 16)))
    down_weight = scatter_about(splits[15], (EXPERTS, FF, D), (FF // 4) ** -0.5, 0.1875, ((0, 16), (1, 16)))
    return {"residual": residual, "queries": queries, "query_rope": query_rope, "latent": latent, "key_rope": key_rope, "latent_gain": latent_gain, "key_weight": key_weight, "value_weight": value_weight, "out_weight": out_weight, "norm_gain": norm_gain, "routes": routes, "group_gate": group_gate, "expert_share": expert_share, "gate_weight": gate_weight, "up_weight": up_weight, "down_weight": down_weight}


rope_base = 10000.0
epsilon = 1e-06

def angle_tables(places, rope_width):
    frequencies = rope_base ** (-jnp.arange(0, rope_width, 2, dtype=jnp.float32) / rope_width)
    angles = places[:, None] * frequencies[None, :]
    return (jnp.cos(angles), jnp.sin(angles))

def rope_turn(values, cosine, sine_table):
    half_size = values.shape[-1] // 2
    first_half = values[..., :half_size]
    second = values[..., half_size:]
    return jnp.concatenate([first_half * cosine - second * sine_table, second * cosine + first_half * sine_table], axis=-1)

def rms_scale(values, gain_vector):
    values = values.astype(jnp.float32)
    inverse = lax.rsqrt(lax.optimization_barrier(jnp.mean(values * values, axis=-1, keepdims=True)) + epsilon)
    return values * inverse * gain_vector.astype(jnp.float32)

def group_attend(query_nope, query_turned, key_nope, rotated_key, value_part, visible, scale):
    scores = jnp.einsum('qhd,khd->hqk', query_nope.astype(jnp.float32), key_nope.astype(jnp.float32))
    scores = scores + jnp.einsum('qhd,kd->hqk', query_turned.astype(jnp.float32), rotated_key.astype(jnp.float32))
    scores = scores * scale
    masked = jnp.where(visible[None], scores, -jnp.inf)
    row_top = lax.optimization_barrier(jnp.max(masked, axis=2, keepdims=True))
    weights = jnp.exp(masked - row_top)
    weight_sum = lax.optimization_barrier(jnp.sum(weights, axis=2))
    rounded = lax.optimization_barrier(weights.astype(jnp.bfloat16)).astype(jnp.float32)
    mixed_rows = jnp.einsum('hqk,khd->qhd', rounded, value_part.astype(jnp.float32))
    return (mixed_rows / jnp.transpose(weight_sum)[:, :, None]).astype(jnp.bfloat16)

def reference(residual, queries, query_rope, latent, key_rope, latent_gain, key_weight, value_weight, out_weight, norm_gain, routes, group_gate, expert_share, gate_weight, up_weight, down_weight):
    places = jnp.arange(SEQ, dtype=jnp.int32).astype(jnp.float32)
    cosine, sine_table = angle_tables(places, DR)
    compressed = rms_scale(latent, latent_gain).astype(jnp.bfloat16)
    rotated_key = rope_turn(key_rope.astype(jnp.float32), cosine, sine_table).astype(jnp.bfloat16)
    turned = rope_turn(query_rope.astype(jnp.float32).reshape(SEQ, PAIRS, 2, DR), cosine[:, None, None, :], sine_table[:, None, None, :]).astype(jnp.bfloat16)
    key_rows = jnp.dot(compressed, key_weight.reshape(LATENT, -1), preferred_element_type=jnp.float32).astype(jnp.bfloat16).reshape(SEQ, PAIRS, DK_A + DK_B)
    value_rows = jnp.dot(compressed, value_weight.reshape(LATENT, -1), preferred_element_type=jnp.float32).astype(jnp.bfloat16).reshape(SEQ, PAIRS, DV_A + DV_B)
    scale_one = (DK_A + DR) ** (-0.5)
    scale_two = (DK_B + DR) ** (-0.5)
    block_size = 256

    def attend_block(block_index):
        block_start = block_index * block_size
        query_block = lax.dynamic_slice_in_dim(queries, block_start, block_size, 0)
        turned_block = lax.dynamic_slice_in_dim(turned, block_start, block_size, 0)
        query_places = (block_start + jnp.arange(block_size, dtype=jnp.int32)).astype(jnp.float32)
        visible = query_places[:, None] >= places[None, :]
        part_one = group_attend(query_block[:, :, :DK_A], turned_block[:, :, 0], key_rows[:, :, :DK_A], rotated_key, value_rows[:, :, :DV_A], visible, scale_one)
        part_two = group_attend(query_block[:, :, DK_A:], turned_block[:, :, 1], key_rows[:, :, DK_A:], rotated_key, value_rows[:, :, DV_A:], visible, scale_two)
        return jnp.concatenate([part_one, part_two], axis=2)
    attention = lax.map(attend_block, jnp.arange(SEQ // block_size, dtype=jnp.int32)).reshape(SEQ, PAIRS * (DV_A + DV_B))
    out_flat = out_weight.reshape(PAIRS * (DV_A + DV_B), D)
    run_width = PAIR_DEV * (DV_A + DV_B)

    def add_run(running, run_index):
        columns = lax.dynamic_slice_in_dim(attention, run_index * run_width, run_width, 1)
        weight_rows = lax.dynamic_slice_in_dim(out_flat, run_index * run_width, run_width, 0)
        partial_sum = jnp.dot(columns, weight_rows, preferred_element_type=jnp.float32)
        return (running + lax.optimization_barrier(partial_sum.astype(jnp.bfloat16)).astype(jnp.float32), None)
    head_total, unused = lax.scan(add_run, jnp.zeros((SEQ, D), jnp.float32), jnp.arange(N_TP, dtype=jnp.int32))
    mixed_rows = residual.astype(jnp.float32) + head_total
    normed = rms_scale(mixed_rows, norm_gain).astype(jnp.bfloat16)
    blocks = SEQ // ROWS
    flat_routes = routes.reshape(blocks, ROWS * TOPK)
    onehot = (flat_routes[:, :, None] == jnp.arange(EXPERTS, dtype=jnp.int32)[None, None, :]).astype(jnp.int32)
    rank_within = lax.optimization_barrier(jnp.sum((jnp.cumsum(onehot, axis=1) - onehot) * onehot, axis=2))
    slot_columns = (jnp.arange(blocks, dtype=jnp.int32)[:, None] * CAP + rank_within).reshape(-1).astype(jnp.int32)
    expert_flat = flat_routes.reshape(-1).astype(jnp.int32)
    token_flat = jnp.repeat(jnp.arange(SEQ, dtype=jnp.int32), TOPK)
    token_of = jnp.full((EXPERTS, blocks * CAP), SEQ, dtype=jnp.int32).at[expert_flat, slot_columns].set(token_flat)
    padded = jnp.concatenate([normed, jnp.zeros((1, D), jnp.bfloat16)], axis=0)
    expert_rows = padded[token_of]

    def expert_apply(inputs):
        rows_in, gate_part, up_part, down_part = inputs
        gate_out = jnp.dot(rows_in, gate_part, preferred_element_type=jnp.float32)
        up_out = jnp.dot(rows_in, up_part, preferred_element_type=jnp.float32)
        hidden = (jax.nn.silu(gate_out) * up_out).astype(jnp.bfloat16)
        hidden_runs = hidden.reshape(hidden.shape[0], N_TP, FF_DEV).astype(jnp.float32)
        down_runs = down_part.reshape(N_TP, FF_DEV, D).astype(jnp.float32)
        partial_sum = jnp.einsum('snf,nfd->snd', hidden_runs, down_runs)
        rounded = lax.optimization_barrier(partial_sum.astype(jnp.bfloat16)).astype(jnp.float32)
        return lax.optimization_barrier(jnp.sum(rounded, axis=1)).astype(jnp.bfloat16)
    outputs = lax.map(expert_apply, (expert_rows, gate_weight, up_weight, down_weight))
    picked = outputs[expert_flat, slot_columns].astype(jnp.float32).reshape(SEQ, TOPK, D)
    share_values = expert_share.astype(jnp.float32)
    route_weight = group_gate.astype(jnp.float32)[:, None] * share_values / lax.optimization_barrier(jnp.sum(share_values, axis=1, keepdims=True))
    expert_mix = lax.optimization_barrier(jnp.sum(route_weight[:, :, None] * picked, axis=1))
    return (mixed_rows + expert_mix).astype(jnp.bfloat16)
```

```python
import functools

import jax
import jax.numpy as jnp
from jax import lax
from jax.experimental import pallas as pl
from jax.experimental.pallas import tpu as pltpu
from jax.sharding import Mesh
from jax.sharding import PartitionSpec as P

DK_A = 64
DV_A = 64
SP = ("y", "x")
TP = ("z", "c")
SP_TP = ("y", "x", "z", "c")
MESH = pl.DeviceIdType.MESH
LOG2E = 1.4426950408889634
BF = jnp.bfloat16
F32 = jnp.float32

rope_base = 10000.0
epsilon = 1e-06
floor_score = -1e30

ORDER = (
    (0, 0),
    (0, 1), (0, 3), (1, 0), (3, 0),
    (0, 2), (2, 0),
    (1, 1), (1, 3), (3, 1), (3, 3),
    (1, 2), (3, 2), (2, 1), (2, 3),
    (2, 2),
)
SLOT = {place: k for k, place in enumerate(ORDER)}
HALF = 208
PART = 112


def place():
    return tuple(lax.axis_index(name) for name in ("y", "x", "z", "c"))


def meet(devices):
    barrier = pltpu.get_barrier_semaphore()
    for device in devices:
        pl.semaphore_signal(barrier, inc=1, device_id=device, device_id_type=MESH)
    pl.semaphore_wait(barrier, len(devices))


def attend_kernel(
    q_ref, own_ref, wk_ref, wv_ref, ow_ref, out_ref,
    buf, kta, ktb, vx, acc, top, owp, attx, attr, part,
    far_out, far_in, step_out, step_in,
    ring_send, ring_recv, flip_send, flip_recv, misc_send, misc_recv, z_send, z_recv,
    *, scale_one, scale_two,
):
    y, x, z, c = place()
    partner = (y, x, z, 1 - c)

    def along_a(step):
        return ((y + c * step + 4) % 4, (x + (1 - c) * step + 4) % 4, z, c)

    def along_b(step):
        return ((y + (1 - c) * step + 4) % 4, (x + c * step + 4) % 4, z, c)

    def along_z(step):
        return (y, x, (z + step + 8) % 8, c)

    def slot(da, db):
        first = SLOT[(db % 4, da % 4)]
        second = SLOT[(da % 4, db % 4)]
        return first if first == second else first + c * (second - first)

    meet(
        [partner, along_a(1), along_a(-1), along_b(1), along_b(-1), along_z(1), along_z(-1)]
    )
    start_row = c * HALF
    other_row = (1 - c) * HALF
    counts = {"ring": 0}
    ring = []

    def piece(k, first, size):
        return buf.at[k - 1, pl.ds(pl.multiple_of(start_row + first, 16), size)]

    spans = {None: (0, HALF), 0: (0, PART), 1: (PART, HALF - PART)}

    def send(source, target, device, which=None):
        first, size = spans[which]
        if source is None:
            src = own_ref.at[pl.ds(pl.multiple_of(start_row + first, 16), size)]
        else:
            src = piece(source, first, size)
        copy = pltpu.make_async_remote_copy(
            src_ref=src,
            dst_ref=piece(target, first, size),
            send_sem=ring_send.at[counts["ring"]],
            recv_sem=ring_recv.at[target - 1, which or 0],
            device_id=device,
            device_id_type=MESH,
        )
        ring.append((counts["ring"], size))
        counts["ring"] += 1
        copy.start()

    def arrived(k, which=None):
        first, size = spans[which]
        pltpu.make_async_remote_copy(
            src_ref=piece(k, first, size),
            dst_ref=piece(k, first, size),
            send_sem=ring_send.at[0],
            recv_sem=ring_recv.at[k - 1, which or 0],
            device_id=partner,
            device_id_type=MESH,
        ).wait_recv()

    def flip(k):
        copy = pltpu.make_async_remote_copy(
            src_ref=piece(k, 0, HALF),
            dst_ref=piece(k, 0, HALF),
            send_sem=flip_send.at[k - 1],
            recv_sem=flip_recv.at[k - 1],
            device_id=partner,
            device_id_type=MESH,
        )
        copy.start()

    def flipped(k):
        there = buf.at[k - 1, pl.ds(pl.multiple_of(other_row, 16), HALF)]
        pltpu.make_async_remote_copy(
            src_ref=there, dst_ref=there,
            send_sem=flip_send.at[0], recv_sem=flip_recv.at[k - 1],
            device_id=partner, device_id_type=MESH,
        ).wait_recv()

    for sign in (1, -1):
        send(None, slot(-sign, 0), along_a(sign))
        send(None, slot(0, -sign), along_b(sign))
    weights_over = pltpu.make_async_remote_copy(
        src_ref=ow_ref, dst_ref=owp, send_sem=misc_send.at[0], recv_sem=misc_recv.at[0],
        device_id=partner, device_id_type=MESH,
    )
    weights_over.start()

    kta[96:128] = jnp.zeros((32, 384), BF)
    ktb[224:256] = jnp.zeros((32, 384), BF)
    lanes = lax.broadcasted_iota(jnp.int32, (1, 384), 1)
    ones = jnp.where((lanes == 64) | (lanes == 320), 1.0, 0.0)
    heads = (
        (slice(0, 128), kta, 0, scale_one * LOG2E),
        (slice(128, 384), ktb, 1, scale_two * LOG2E),
    )

    def block(ref, first):
        rope = ref[0:32, 0:384]
        lat = ref[32:416, :]
        keys = lax.dot_general(
            wk_ref[...], lat, (((1,), (1,)), ((), ())), preferred_element_type=F32
        ).astype(BF)
        kta[0:64] = keys[0:64]
        kta[64:96] = rope
        ktb[0:192] = keys[64:256]
        ktb[192:224] = rope
        vx[...] = (jnp.dot(lat, wv_ref[...], preferred_element_type=F32) + ones).astype(BF)
        for cols, keys_ref, h, factor in heads:
            scores = jnp.dot(q_ref[:, cols], keys_ref[...], preferred_element_type=F32)
            if first:
                rows = lax.broadcasted_iota(jnp.int32, (384, 384), 0)
                places = lax.broadcasted_iota(jnp.int32, (384, 384), 1)
                scores = jnp.where(rows >= places, scores, floor_score)
            peak = jnp.max(scores, axis=1, keepdims=True)
            width = (cols.stop - cols.start) // 128
            if first:
                new = jnp.broadcast_to(peak, (384, 128))
            else:
                old = top[h]
                new = jnp.maximum(old, peak)
            top[h] = new
            weights = jnp.exp2(
                (scores - jnp.concatenate([new] * 3, axis=1)) * factor
            ).astype(BF)
            update = jnp.dot(weights, vx[:, cols], preferred_element_type=F32)
            if first:
                acc[:, cols] = update
            else:
                shrink = jnp.exp2((old - new) * factor)
                acc[:, cols] = acc[:, cols] * jnp.concatenate([shrink] * width, axis=1) + update

    block(own_ref, True)

    me = y * 4 + x

    def step(i, carry):
        @pl.when(i == 1)
        def _():
            near = []
            for sign in (1, -1):
                k = slot(-sign, 0)
                arrived(k)
                flip(k)
                send(k, slot(-2 * sign, 0), along_a(sign), 0 if sign == 1 else 1)
                near.append(k)
                k = slot(0, -sign)
                arrived(k)
                flip(k)
                send(k, slot(0, -2 * sign), along_b(sign), 0 if sign == 1 else 1)
            for sign, k in zip((1, -1), near):
                send(k, slot(-sign, -1), along_b(1))
                send(k, slot(-sign, 1), along_b(-1))

        @pl.when(i == 5)
        def _():
            k = slot(2, 0)
            arrived(k, 0)
            arrived(k, 1)
            flip(k)
            send(k, slot(2, -1), along_b(1))
            send(k, slot(2, 1), along_b(-1))
            k = slot(0, 2)
            arrived(k, 0)
            arrived(k, 1)
            flip(k)

        @pl.when(i == 7)
        def _():
            for da in (-1, 1):
                for sign in (1, -1):
                    k = slot(da, -sign)
                    arrived(k)
                    flip(k)
                    send(k, slot(da, -2 * sign), along_b(sign), 0 if sign == 1 else 1)

        @pl.when(i == 11)
        def _():
            for sign in (1, -1):
                k = slot(2, -sign)
                arrived(k)
                flip(k)
                send(k, slot(2, -2 * sign), along_b(sign), 0 if sign == 1 else 1)
            for da in (-1, 1):
                k = slot(da, 2)
                arrived(k, 0)
                arrived(k, 1)
                flip(k)

        @pl.when(i == 15)
        def _():
            k = slot(2, 2)
            arrived(k, 0)
            arrived(k, 1)
            flip(k)

        flipped(i)
        dy = 0
        dx = 0
        for k in range(1, 16):
            dy = jnp.where(i == k, ORDER[k][0], dy)
            dx = jnp.where(i == k, ORDER[k][1], dx)
        theirs = ((y + dy) % 4) * 4 + (x + dx) % 4

        @pl.when(theirs < me)
        def _():
            block(buf.at[i - 1], False)

        return carry

    lax.fori_loop(1, 16, step, 0)

    total = acc[...]
    part_a = total[:, 0:128] / total[:, 64:65]
    part_b = total[:, 128:384] / total[:, 320:321]
    both = jnp.concatenate([part_a, part_b], axis=1)
    for side in (0, 1):
        attx[side] = jnp.concatenate(
            [both[(2 * k + side) * 24 : (2 * k + side + 1) * 24] for k in range(8)], axis=0
        ).astype(BF)
    heads_over = pltpu.make_async_remote_copy(
        src_ref=attx.at[1 - c], dst_ref=attr, send_sem=misc_send.at[1], recv_sem=misc_recv.at[1],
        device_id=partner, device_id_type=MESH,
    )
    heads_over.start()
    weights_over.wait_recv()
    mine = attx[c]
    partial = jnp.dot(mine[:, 0:64], ow_ref[0:64], preferred_element_type=F32)
    partial = partial + jnp.dot(mine[:, 128:320], ow_ref[64:256], preferred_element_type=F32)
    heads_over.wait_recv()
    given = attr[...]
    partial = partial + jnp.dot(given[:, 0:64], owp[0:64], preferred_element_type=F32)
    partial = partial + jnp.dot(given[:, 128:320], owp[64:256], preferred_element_type=F32)
    part[...] = partial.reshape(8, 24, 2048)

    sent = []

    def pass_on(src, dst, sign, k):
        way = 0 if sign == 1 else 1
        copy = pltpu.make_async_remote_copy(
            src_ref=src, dst_ref=dst, send_sem=z_send.at[way, k], recv_sem=z_recv.at[way, k],
            device_id=along_z(sign), device_id_type=MESH,
        )
        copy.start()
        sent.append(copy)
        return copy

    ways = ((1, 0, slice(0, 1024)), (-1, 1, slice(1024, 2048)))
    pending = {}
    for sign, way, cols in ways:
        far_out[way] = part[(z + 4) % 8, :, cols].astype(BF)
        pending[sign] = pass_on(far_out.at[way], far_in.at[way], sign, 0)
    for hop in (1, 2, 3):
        for sign, way, cols in ways:
            pending[sign].wait_recv()
            mine = part.at[(z + sign * (4 - hop) + 8) % 8]
            if hop == 1:
                inside = mine[:, cols] + far_in[way].astype(F32)
                outside = mine[:, 1024:2048] if way == 0 else mine[:, 0:1024]
                pair = [inside, outside] if way == 0 else [outside, inside]
                value = jnp.concatenate(pair, axis=1)
            else:
                value = mine[...] + step_in[way, hop - 2].astype(F32)
            step_out[way, hop - 1] = value.astype(BF)
            pending[sign] = pass_on(
                step_out.at[way, hop - 1], step_in.at[way, hop - 1], sign, hop
            )
    pending[1].wait_recv()
    pending[-1].wait_recv()
    out_ref[...] = part[z] + step_in[0, 2].astype(F32) + step_in[1, 2].astype(F32)

    ends = [(ring_send.at[k], size) for k, size in ring]
    ends += [(flip_send.at[k], HALF) for k in range(15)]
    for sem, size in ends:
        pltpu.make_async_remote_copy(
            src_ref=buf.at[0, pl.ds(0, size)], dst_ref=buf.at[0, pl.ds(0, size)],
            send_sem=sem, recv_sem=flip_recv.at[0], device_id=partner, device_id_type=MESH,
        ).wait_send()
    for copy in sent + [weights_over, heads_over]:
        copy.wait_send()


def head_sums(q_ext, own, wk, wv, ow, scale_one, scale_two):
    vmem = pl.BlockSpec(memory_space=pltpu.VMEM)
    return pl.pallas_call(
        functools.partial(attend_kernel, scale_one=scale_one, scale_two=scale_two),
        out_shape=jax.ShapeDtypeStruct((24, 2048), F32),
        in_specs=[vmem] * 5,
        out_specs=vmem,
        scratch_shapes=[
            pltpu.VMEM((15, 416, 512), BF),
            pltpu.VMEM((128, 384), BF),
            pltpu.VMEM((256, 384), BF),
            pltpu.VMEM((384, 384), BF),
            pltpu.VMEM((384, 384), F32),
            pltpu.VMEM((2, 384, 128), F32),
            pltpu.VMEM((256, 2048), BF),
            pltpu.VMEM((2, 192, 384), BF),
            pltpu.VMEM((192, 384), BF),
            pltpu.VMEM((8, 24, 2048), F32),
            pltpu.VMEM((2, 24, 1024), BF),
            pltpu.VMEM((2, 24, 1024), BF),
            pltpu.VMEM((2, 3, 24, 2048), BF),
            pltpu.VMEM((2, 3, 24, 2048), BF),
            pltpu.SemaphoreType.DMA((20,)),
            pltpu.SemaphoreType.DMA((15, 2)),
            pltpu.SemaphoreType.DMA((15,)),
            pltpu.SemaphoreType.DMA((15,)),
            pltpu.SemaphoreType.DMA((2,)),
            pltpu.SemaphoreType.DMA((2,)),
            pltpu.SemaphoreType.DMA((2, 4)),
            pltpu.SemaphoreType.DMA((2, 4)),
        ],
        compiler_params=pltpu.CompilerParams(
            collective_id=0, has_side_effects=True, vmem_limit_bytes=60 * 1024 * 1024
        ),
        name="attend",
    )(q_ext, own, wk, wv, ow)


def in_blocks(value, dim, count):
    dims = value.shape
    pieces = value.reshape(*dims[:dim], count, dims[dim] // count, *dims[dim + 1 :])
    return jnp.moveaxis(pieces, dim, 0)


def sum_at_owner(value, axis, dim):
    pieces = in_blocks(value, dim, lax.axis_size(axis))
    arrived = lax.all_to_all(pieces, axis, split_axis=0, concat_axis=0, tiled=True)
    return arrived.astype(jnp.float32).sum(axis=0)


def laid_out(pieces, dim):
    dims = list(pieces.shape[1:])
    dims[dim] *= pieces.shape[0]
    return jnp.moveaxis(pieces, 0, dim).reshape(dims)


def turned_blocks(pieces, axes, sequence):
    inside = pieces.shape[1:]
    out = pieces.reshape(*(lax.axis_size(a) for a in axes), *inside)
    for k in sequence:
        out = lax.all_to_all(out, axes[k], k, k, tiled=True)
    return out.reshape(-1, *inside)


def stepwise_exchange(value, axes, sequence, split_dim, concat_dim):
    pieces = in_blocks(value, split_dim, lax.axis_size(axes))
    return laid_out(turned_blocks(pieces, axes, sequence), concat_dim)


def angle_tables(places, rope_width):
    frequencies = rope_base ** (-jnp.arange(0, rope_width, 2, dtype=jnp.float32) / rope_width)
    angles = places[:, None] * frequencies[None, :]
    return (jnp.cos(angles), jnp.sin(angles))


def rope_turn(values, cosine, sine_table):
    half_size = values.shape[-1] // 2
    first_half = values[..., :half_size]
    second = values[..., half_size:]
    return jnp.concatenate(
        [first_half * cosine - second * sine_table, second * cosine + first_half * sine_table],
        axis=-1,
    )


def rms_scale(values, gain_vector):
    values = values.astype(jnp.float32)
    inverse = lax.rsqrt(jnp.mean(values * values, axis=-1, keepdims=True) + epsilon)
    return values * inverse * gain_vector


def slot_table(route_block, experts_all, capacity):
    flat_routes = route_block.reshape(-1)
    onehot = (flat_routes[:, None] == jnp.arange(experts_all, dtype=jnp.int32)[None, :]).astype(
        jnp.int32
    )
    rank_within = jnp.sum((jnp.cumsum(onehot, axis=0) - onehot) * onehot, axis=1)
    return flat_routes * capacity + rank_within


def local(
    residual,
    queries,
    query_rope,
    latent,
    key_rope,
    latent_gain,
    key_weight,
    value_weight,
    out_weight,
    norm_gain,
    routes,
    group_gate,
    expert_share,
    gate_weight,
    up_weight,
    down_weight,
):
    local_tokens = queries.shape[0]
    pair_dev = queries.shape[1]
    sp_count = lax.axis_size(SP)
    tp_count = lax.axis_size(TP)
    row_count = local_tokens // tp_count
    rope_width = key_rope.shape[1]
    first_place = lax.axis_index(SP) * local_tokens
    places = (first_place + jnp.arange(local_tokens, dtype=jnp.int32)).astype(jnp.float32)
    cosine, sine_table = angle_tables(places, rope_width)
    rotated_key = rope_turn(key_rope.astype(jnp.float32), cosine, sine_table).astype(jnp.bfloat16)
    turned = rope_turn(
        query_rope.astype(jnp.float32).reshape(local_tokens, pair_dev, 2, rope_width),
        cosine[:, None, None, :],
        sine_table[:, None, None, :],
    ).astype(jnp.bfloat16)
    compressed = rms_scale(latent, latent_gain).astype(BF)
    scale_one = (DK_A + rope_width) ** (-0.5)
    scale_two = (queries.shape[2] - DK_A + rope_width) ** (-0.5)
    own = jnp.concatenate(
        [jnp.pad(rotated_key.T, ((0, 0), (0, 128))), compressed], axis=0
    )
    flat = queries[:, 0]
    blank = jnp.zeros((local_tokens, 32), BF)
    q_ext = jnp.concatenate(
        [flat[:, :DK_A], turned[:, 0, 0], blank, flat[:, DK_A:], turned[:, 0, 1], blank], axis=1
    )
    key_flat = key_weight[:, 0].T
    value_flat = value_weight[:, 0]
    zeros = jnp.zeros((value_flat.shape[0], 64), BF)
    value_ext = jnp.concatenate(
        [value_flat[:, :DV_A], zeros, value_flat[:, DV_A:], zeros], axis=1
    )
    head_total = head_sums(
        q_ext, own, key_flat, value_ext, out_weight[0], scale_one, scale_two
    )
    mixed_rows = residual.astype(jnp.float32) + head_total
    normed = rms_scale(mixed_rows, norm_gain).astype(jnp.bfloat16)
    experts_dev = gate_weight.shape[0]
    experts_all = experts_dev * sp_count
    top_count = routes.shape[1]
    capacity = max(2, 3 * row_count * top_count // (2 * experts_all))
    slot_count = experts_all * capacity
    own_routes = lax.dynamic_slice_in_dim(routes, lax.axis_index(TP) * row_count, row_count, 0)
    own_slots = slot_table(own_routes, experts_all, capacity)
    pick_matrix = (jnp.arange(slot_count, dtype=jnp.int32)[:, None] == own_slots[None, :]).astype(
        jnp.bfloat16
    )
    pick_matrix = pick_matrix.reshape(slot_count, row_count, top_count).sum(axis=2)
    outgoing = (
        jnp.dot(pick_matrix, normed, preferred_element_type=jnp.float32)
        .astype(jnp.bfloat16)
        .reshape(sp_count, experts_dev, capacity, -1)
    )
    arrived = stepwise_exchange(outgoing, SP, (0, 1), 0, 0)
    gathered = lax.all_gather(arrived, TP, axis=0, tiled=True)
    gate_out = jnp.einsum(
        "secd,edf->secf", gathered, gate_weight, preferred_element_type=jnp.float32
    )
    up_out = jnp.einsum("secd,edf->secf", gathered, up_weight, preferred_element_type=jnp.float32)
    hidden = (jax.nn.silu(gate_out) * up_out).astype(jnp.bfloat16)
    expert_out = lax.psum_scatter(
        jnp.einsum(
            "secf,efd->secd", hidden, down_weight, preferred_element_type=jnp.float32
        ).astype(jnp.bfloat16),
        TP,
        scatter_dimension=0,
        tiled=True,
    )
    returned = lax.all_to_all(expert_out, SP, split_axis=0, concat_axis=0, tiled=True).reshape(
        slot_count, -1
    )
    selectors = (own_slots[:, None] == jnp.arange(slot_count, dtype=jnp.int32)[None, :]).astype(
        jnp.bfloat16
    )
    picked = jnp.dot(selectors, returned, preferred_element_type=jnp.float32).reshape(
        row_count, top_count, -1
    )
    route_weight = group_gate[:, None] * expert_share / jnp.sum(expert_share, axis=1, keepdims=True)
    expert_mix = jnp.sum(route_weight[:, :, None] * picked, axis=1)
    return (mixed_rows + expert_mix).astype(jnp.bfloat16)


def solution(mesh):
    finer = Mesh(mesh.devices.reshape(4, 4, 8, 2), ("y", "x", "z", "c"))
    placed = (
        P(SP_TP, None),
        P(SP, TP, None),
        P(SP, TP, None),
        P(SP, None),
        P(SP, None),
        P(),
        P(None, TP, None),
        P(None, TP, None),
        P(TP, None, None),
        P(),
        P(SP, None),
        P(SP_TP),
        P(SP_TP, None),
        P(SP, None, TP),
        P(SP, None, TP),
        P(SP, TP, None),
    )
    return jax.shard_map(
        local, mesh=finer, in_specs=placed, out_specs=P(SP_TP, None), check_vma=False
    )
```

```python
import functools

import jax
import jax.numpy as jnp
from jax import lax
from jax.experimental import pallas as pl
from jax.experimental.pallas import tpu as pltpu
from jax.sharding import Mesh
from jax.sharding import PartitionSpec as P

DK_A = 64
DV_A = 64
SP = ("y", "x")
TP = ("z", "c")
SP_TP = ("y", "x", "z", "c")
MESH = pl.DeviceIdType.MESH
LOG2E = 1.4426950408889634
BF = jnp.bfloat16
F32 = jnp.float32

rope_base = 10000.0
epsilon = 1e-06
floor_score = -1e30

ORDER = (
    (0, 0),
    (0, 1), (0, 3), (1, 0), (3, 0),
    (0, 2), (2, 0),
    (1, 1), (1, 3), (3, 1), (3, 3),
    (1, 2), (3, 2), (2, 1), (2, 3),
    (2, 2),
)
SLOT = {place: k for k, place in enumerate(ORDER)}
HALF = 208
PART = 112


def place():
    return tuple(lax.axis_index(name) for name in ("y", "x", "z", "c"))


def meet(devices):
    barrier = pltpu.get_barrier_semaphore()
    for device in devices:
        pl.semaphore_signal(barrier, inc=1, device_id=device, device_id_type=MESH)
    pl.semaphore_wait(barrier, len(devices))


DZ = (0, -1, 1, -2, 2, -3, 3, 4)
BASE = {dz: 2 * k for k, dz in enumerate(DZ)}


def spread_place(column):
    return column + jnp.where(column >= DK_A, 64, 0)


def chosen(condition):
    return jnp.where(condition, 1.0, 0.0).astype(BF)


def layer_kernel(
    q_ref, turned_ref, own_ref, wk_ref, wv_ref, ow_ref, residual_ref, gain_ref,
    slots_ref, spots_ref, share_ref, gate_hbm, up_hbm, down_hbm, out_ref,
    qx, wkt, wvx, buf, kta, ktb, vx, acc, top, owp, attx, attr, part,
    far_out, far_in, step_out, step_in, mixed_ref, disp, arr, rows_ref,
    held, gate, up, down, made, given, rs_out, rs_in, sums_ref, ret, back,
    ring_send, ring_recv, flip_send, flip_recv, misc_send, misc_recv, head_send, head_recv,
    disp_send, disp_recv, load_sem, z_send, z_recv, swap_send, swap_recv,
    give_send, give_recv, rs_send, rs_recv, back_send, back_recv,
    *, scale_one, scale_two,
):
    y, x, z, c = place()
    partner = (y, x, z, 1 - c)

    def along_a(step):
        return ((y + c * step + 4) % 4, (x + (1 - c) * step + 4) % 4, z, c)

    def along_b(step):
        return ((y + (1 - c) * step + 4) % 4, (x + c * step + 4) % 4, z, c)

    def along_z(step):
        return (y, x, (z + step + 8) % 8, c)

    def slot(da, db):
        first = SLOT[(db % 4, da % 4)]
        second = SLOT[(da % 4, db % 4)]
        return first if first == second else first + c * (second - first)

    me = y * 4 + x
    peers = [
        (dy, dx, ((y + dy) % 4, (x + dx) % 4, z, c))
        for dy in range(4) for dx in range(4) if dy or dx
    ]
    loads = [
        pltpu.make_async_copy(src, dst, load_sem.at[k])
        for k, (src, dst) in enumerate(((gate_hbm, gate), (up_hbm, up), (down_hbm, down)))
    ]
    for load in loads:
        load.start()
    meet([partner, along_z(1), along_z(-1)] + [peer[2] for peer in peers])
    start_row = c * HALF
    other_row = (1 - c) * HALF
    counts = {"ring": 0}
    ring = []

    def piece(k, first, size):
        return buf.at[k - 1, pl.ds(pl.multiple_of(start_row + first, 16), size)]

    spans = {None: (0, HALF), 0: (0, PART), 1: (PART, HALF - PART)}

    def send(source, target, device, which=None):
        first, size = spans[which]
        if source is None:
            src = own_ref.at[pl.ds(pl.multiple_of(start_row + first, 16), size)]
        else:
            src = piece(source, first, size)
        copy = pltpu.make_async_remote_copy(
            src_ref=src,
            dst_ref=piece(target, first, size),
            send_sem=ring_send.at[counts["ring"]],
            recv_sem=ring_recv.at[target - 1, which or 0],
            device_id=device,
            device_id_type=MESH,
        )
        ring.append((counts["ring"], size))
        counts["ring"] += 1
        copy.start()

    def arrived(k, which=None):
        first, size = spans[which]
        pltpu.make_async_remote_copy(
            src_ref=piece(k, first, size),
            dst_ref=piece(k, first, size),
            send_sem=ring_send.at[0],
            recv_sem=ring_recv.at[k - 1, which or 0],
            device_id=partner,
            device_id_type=MESH,
        ).wait_recv()

    def flip(k):
        copy = pltpu.make_async_remote_copy(
            src_ref=piece(k, 0, HALF),
            dst_ref=piece(k, 0, HALF),
            send_sem=flip_send.at[k - 1],
            recv_sem=flip_recv.at[k - 1],
            device_id=partner,
            device_id_type=MESH,
        )
        copy.start()

    def flipped(k):
        there = buf.at[k - 1, pl.ds(pl.multiple_of(other_row, 16), HALF)]
        pltpu.make_async_remote_copy(
            src_ref=there, dst_ref=there,
            send_sem=flip_send.at[0], recv_sem=flip_recv.at[k - 1],
            device_id=partner, device_id_type=MESH,
        ).wait_recv()

    for sign in (1, -1):
        send(None, slot(-sign, 0), along_a(sign))
        send(None, slot(0, -sign), along_b(sign))
    weights_over = pltpu.make_async_remote_copy(
        src_ref=ow_ref, dst_ref=owp, send_sem=misc_send.at[0], recv_sem=misc_recv.at[0],
        device_id=partner, device_id_type=MESH,
    )
    weights_over.start()

    spread = chosen(
        lax.broadcasted_iota(jnp.int32, (256, 384), 1)
        == spread_place(lax.broadcasted_iota(jnp.int32, (256, 384), 0))
    )
    turns = lax.broadcasted_iota(jnp.int32, (64, 384), 0)
    turns = chosen(
        lax.broadcasted_iota(jnp.int32, (64, 384), 1)
        == turns + 64 + jnp.where(turns >= 32, 224, 0)
    )
    qx[...] = (
        jnp.dot(q_ref[...], spread, preferred_element_type=F32)
        + jnp.dot(turned_ref[...], turns, preferred_element_type=F32)
    ).astype(BF)
    wvx[...] = jnp.dot(wv_ref[...], spread, preferred_element_type=F32).astype(BF)
    unit = chosen(
        lax.broadcasted_iota(jnp.int32, (256, 256), 0)
        == lax.broadcasted_iota(jnp.int32, (256, 256), 1)
    )
    wkt[...] = lax.dot_general(
        unit, wk_ref[...], (((1,), (1,)), ((), ())), preferred_element_type=F32
    ).astype(BF)
    kta[96:128] = jnp.zeros((32, 384), BF)
    ktb[224:256] = jnp.zeros((32, 384), BF)
    lanes = lax.broadcasted_iota(jnp.int32, (1, 384), 1)
    ones = jnp.where((lanes == 64) | (lanes == 320), 1.0, 0.0)
    heads = (
        (slice(0, 128), kta, 0, scale_one * LOG2E),
        (slice(128, 384), ktb, 1, scale_two * LOG2E),
    )

    def block(ref, first):
        rope = ref[0:32, 0:384]
        lat = ref[32:416, :]
        keys = lax.dot_general(
            wkt[...], lat, (((1,), (1,)), ((), ())), preferred_element_type=F32
        ).astype(BF)
        kta[0:64] = keys[0:64]
        kta[64:96] = rope
        ktb[0:192] = keys[64:256]
        ktb[192:224] = rope
        vx[...] = (jnp.dot(lat, wvx[...], preferred_element_type=F32) + ones).astype(BF)
        for cols, keys_ref, h, factor in heads:
            scores = jnp.dot(qx[:, cols], keys_ref[...], preferred_element_type=F32)
            if first:
                rows = lax.broadcasted_iota(jnp.int32, (384, 384), 0)
                places = lax.broadcasted_iota(jnp.int32, (384, 384), 1)
                scores = jnp.where(rows >= places, scores, floor_score)
            peak = jnp.max(scores, axis=1, keepdims=True)
            width = (cols.stop - cols.start) // 128
            if first:
                new = jnp.broadcast_to(peak, (384, 128))
            else:
                old = top[h]
                new = jnp.maximum(old, peak)
            top[h] = new
            weights = jnp.exp2(
                (scores - jnp.concatenate([new] * 3, axis=1)) * factor
            ).astype(BF)
            update = jnp.dot(weights, vx[:, cols], preferred_element_type=F32)
            if first:
                acc[:, cols] = update
            else:
                shrink = jnp.exp2((old - new) * factor)
                acc[:, cols] = acc[:, cols] * jnp.concatenate([shrink] * width, axis=1) + update

    block(own_ref, True)

    def step(i, carry):
        @pl.when(i == 1)
        def _():
            near = []
            for sign in (1, -1):
                k = slot(-sign, 0)
                arrived(k)
                flip(k)
                send(k, slot(-2 * sign, 0), along_a(sign), 0 if sign == 1 else 1)
                near.append(k)
                k = slot(0, -sign)
                arrived(k)
                flip(k)
                send(k, slot(0, -2 * sign), along_b(sign), 0 if sign == 1 else 1)
            for sign, k in zip((1, -1), near):
                send(k, slot(-sign, -1), along_b(1))
                send(k, slot(-sign, 1), along_b(-1))

        @pl.when(i == 5)
        def _():
            k = slot(2, 0)
            arrived(k, 0)
            arrived(k, 1)
            flip(k)
            send(k, slot(2, -1), along_b(1))
            send(k, slot(2, 1), along_b(-1))
            k = slot(0, 2)
            arrived(k, 0)
            arrived(k, 1)
            flip(k)

        @pl.when(i == 7)
        def _():
            for da in (-1, 1):
                for sign in (1, -1):
                    k = slot(da, -sign)
                    arrived(k)
                    flip(k)
                    send(k, slot(da, -2 * sign), along_b(sign), 0 if sign == 1 else 1)

        @pl.when(i == 11)
        def _():
            for sign in (1, -1):
                k = slot(2, -sign)
                arrived(k)
                flip(k)
                send(k, slot(2, -2 * sign), along_b(sign), 0 if sign == 1 else 1)
            for da in (-1, 1):
                k = slot(da, 2)
                arrived(k, 0)
                arrived(k, 1)
                flip(k)

        @pl.when(i == 15)
        def _():
            k = slot(2, 2)
            arrived(k, 0)
            arrived(k, 1)
            flip(k)

        flipped(i)
        dy = 0
        dx = 0
        for k in range(1, 16):
            dy = jnp.where(i == k, ORDER[k][0], dy)
            dx = jnp.where(i == k, ORDER[k][1], dx)
        theirs = ((y + dy) % 4) * 4 + (x + dx) % 4

        @pl.when(theirs < me)
        def _():
            block(buf.at[i - 1], False)

        return carry

    lax.fori_loop(1, 16, step, 0)

    total = acc[...]
    part_a = total[:, 0:128] / total[:, 64:65]
    part_b = total[:, 128:384] / total[:, 320:321]
    both = jnp.concatenate([part_a, part_b], axis=1)
    for side in (0, 1):
        attx[side] = jnp.concatenate(
            [both[(2 * k + side) * 24 : (2 * k + side + 1) * 24] for k in range(8)], axis=0
        ).astype(BF)
    heads_over = pltpu.make_async_remote_copy(
        src_ref=attx.at[1 - c], dst_ref=attr, send_sem=misc_send.at[1], recv_sem=misc_recv.at[1],
        device_id=partner, device_id_type=MESH,
    )
    heads_over.start()
    weights_over.wait_recv()
    mine = attx[c]
    partial = jnp.dot(mine[:, 0:64], ow_ref[0:64], preferred_element_type=F32)
    partial = partial + jnp.dot(mine[:, 128:320], ow_ref[64:256], preferred_element_type=F32)
    heads_over.wait_recv()
    theirs = attr[...]
    partial = partial + jnp.dot(theirs[:, 0:64], owp[0:64], preferred_element_type=F32)
    partial = partial + jnp.dot(theirs[:, 128:320], owp[64:256], preferred_element_type=F32)
    part[...] = partial.reshape(8, 24, 2048)

    sent = []

    def pass_on(src, dst, sign, k):
        way = 0 if sign == 1 else 1
        copy = pltpu.make_async_remote_copy(
            src_ref=src, dst_ref=dst, send_sem=head_send.at[way, k], recv_sem=head_recv.at[way, k],
            device_id=along_z(sign), device_id_type=MESH,
        )
        copy.start()
        sent.append(copy)
        return copy

    ways = ((1, 0, slice(0, 1024)), (-1, 1, slice(1024, 2048)))
    pending = {}
    for sign, way, cols in ways:
        far_out[way] = part[(z + 4) % 8, :, cols].astype(BF)
        pending[sign] = pass_on(far_out.at[way], far_in.at[way], sign, 0)
    for hop in (1, 2, 3):
        for sign, way, cols in ways:
            pending[sign].wait_recv()
            mine = part.at[(z + sign * (4 - hop) + 8) % 8]
            if hop == 1:
                inside = mine[:, cols] + far_in[way].astype(F32)
                outside = mine[:, 1024:2048] if way == 0 else mine[:, 0:1024]
                pair = [inside, outside] if way == 0 else [outside, inside]
                value = jnp.concatenate(pair, axis=1)
            else:
                value = mine[...] + step_in[way, hop - 2].astype(F32)
            step_out[way, hop - 1] = value.astype(BF)
            pending[sign] = pass_on(
                step_out.at[way, hop - 1], step_in.at[way, hop - 1], sign, hop
            )
    pending[1].wait_recv()
    pending[-1].wait_recv()
    mixed = residual_ref[...].astype(F32) + part[z]
    mixed = mixed + step_in[0, 2].astype(F32) + step_in[1, 2].astype(F32)
    mixed_ref[...] = mixed
    inverse = lax.rsqrt(jnp.mean(mixed * mixed, axis=1, keepdims=True) + epsilon)
    normed = mixed * inverse * gain_ref[...]
    stack = jnp.concatenate([normed[:, j * 512 : (j + 1) * 512] for j in range(4)], axis=0)
    rows = lax.broadcasted_iota(jnp.int32, (256, 96), 0)
    columns = lax.broadcasted_iota(jnp.int32, (256, 96), 1)
    wanted = (rows // 16) * 4 + rows % 4
    hit = (wanted == slots_ref[0:1, :]) | (wanted == slots_ref[1:2, :])
    pick = chosen(hit & ((rows // 4) % 4 == columns // 24))
    outgoing = jnp.dot(pick, stack.astype(BF), preferred_element_type=F32).astype(BF)
    disp[...] = outgoing.reshape(16, 16, 512)

    def exchange(source, target, send_sem, recv_sem):
        target[me] = source[me]
        moves = []
        for dy, dx, peer in peers:
            there = peer[0] * 4 + peer[1]
            k = dy * 4 + dx - 1
            copy = pltpu.make_async_remote_copy(
                src_ref=source.at[there], dst_ref=target.at[me],
                send_sem=send_sem.at[k], recv_sem=recv_sem.at[k],
                device_id=peer, device_id_type=MESH,
            )
            copy.start()
            moves.append(copy)
        for copy in moves:
            copy.wait_recv()
        return moves

    moves = exchange(disp, arr, disp_send, disp_recv)
    order = lax.broadcasted_iota(jnp.int32, (256, 256), 0)
    order = ((order // 2) % 16) * 16 + (order // 64) * 4 + ((order // 32) % 2) * 2 + order % 2
    unpack = chosen(lax.broadcasted_iota(jnp.int32, (256, 256), 1) == order)
    arrived_rows = jnp.dot(
        unpack, arr[...].reshape(256, 512), preferred_element_type=F32
    ).astype(BF)
    for j in range(4):
        piece_rows = arrived_rows[j * 64 : (j + 1) * 64].reshape(2, 32, 512)
        rows_ref[:, :, j * 512 : (j + 1) * 512] = piece_rows

    copies = []

    def remote(src, dst, send_sem, recv_sem, device):
        copy = pltpu.make_async_remote_copy(
            src_ref=src, dst_ref=dst, send_sem=send_sem, recv_sem=recv_sem,
            device_id=device, device_id_type=MESH,
        )
        copy.start()
        copies.append(copy)
        return copy

    hops = {}
    flips = {}
    for e in (0, 1):
        for way, sign in ((0, 1), (1, -1)):
            hops[way, 1, e] = remote(
                rows_ref.at[e], held.at[e, BASE[-sign] + c],
                z_send.at[way, 0, e], z_recv.at[way, 0, e], along_z(sign),
            )
        flips[0, e] = remote(
            rows_ref.at[e], held.at[e, c], swap_send.at[0, e], swap_recv.at[0, e], partner
        )
        held[e, c] = rows_ref[e]

    def compute(first, count, dzs):
        for e in (0, 1):
            rows = held[e, first : first + count].reshape(count * 32, 2048)
            inner = jnp.dot(rows, gate[e], preferred_element_type=F32)
            inner = inner / (1.0 + jnp.exp(-inner))
            inner = inner * jnp.dot(rows, up[e], preferred_element_type=F32)
            result = jnp.dot(inner.astype(BF), down[e], preferred_element_type=F32)
            made[e, first : first + count] = result.astype(BF).reshape(count, 32, 2048)
            for dz in dzs:
                k = BASE[dz] // 2
                gives[dz, e] = remote(
                    made.at[e, BASE[dz] + 1 - c], given.at[e, k],
                    give_send.at[k, e], give_recv.at[k, e], partner,
                )

    gives = {}

    def chip_sum(dz, e):
        if (dz, e) in gives:
            gives.pop((dz, e)).wait_recv()
        return made[e, BASE[dz] + c].astype(F32) + given[e, BASE[dz] // 2].astype(F32)

    for load in loads:
        load.wait()
    for e in (0, 1):
        flips[0, e].wait_recv()
    compute(0, 2, (0,))
    for dist in (1, 2, 3):
        for e in (0, 1):
            for way, sign in ((0, 1), (1, -1)):
                hops[way, dist, e].wait_recv()
                dz = -sign * dist
                spot = held.at[e, BASE[dz] + c]
                k = BASE[dz] // 2
                if dist < 3:
                    target = held.at[e, BASE[dz - sign] + c]
                elif way == e:
                    target = held.at[e, BASE[4] + c]
                else:
                    target = None
                if target is not None:
                    hops[way, dist + 1, e] = remote(
                        spot, target, z_send.at[way, dist, e], z_recv.at[way, dist, e],
                        along_z(sign),
                    )
                flips[k, e] = remote(
                    spot, spot, swap_send.at[k, e], swap_recv.at[k, e], partner
                )
        for e in (0, 1):
            for dz in (-dist, dist):
                flips[BASE[dz] // 2, e].wait_recv()
        compute(4 * dist - 2, 4, (-dist, dist))

    sums = {}

    def push(way, e, hop, value):
        sign = 1 if way == 0 else -1
        rs_out[way, e, hop] = value.astype(BF)
        sums[way, e] = remote(
            rs_out.at[way, e, hop], rs_in.at[way, e, hop],
            rs_send.at[way, e, hop], rs_recv.at[way, e, hop], along_z(sign),
        )

    push(0, 1, 1, chip_sum(3, 1))
    push(1, 0, 1, chip_sum(-3, 0))
    for e in (0, 1):
        hops[e, 4, e].wait_recv()
        spot = held.at[e, BASE[4] + c]
        flips[7, e] = remote(spot, spot, swap_send.at[7, e], swap_recv.at[7, e], partner)
    for e in (0, 1):
        flips[7, e].wait_recv()
    compute(14, 2, (4,))
    push(0, 0, 0, chip_sum(4, 0))
    push(1, 1, 0, chip_sum(4, 1))
    for hop in (1, 2, 3):
        if hop < 3:
            for way, e in ((0, 1), (1, 0)):
                sums[way, e].wait_recv()
                dz = (3 - hop) * (1 if way == 0 else -1)
                push(way, e, hop + 1, chip_sum(dz, e) + rs_in[way, e, hop].astype(F32))
        for way, e in ((0, 0), (1, 1)):
            sums[way, e].wait_recv()
            dz = (4 - hop) * (1 if way == 0 else -1)
            push(way, e, hop, chip_sum(dz, e) + rs_in[way, e, hop - 1].astype(F32))
    for e in (0, 1):
        own = chip_sum(0, e)
        for way in (0, 1):
            sums[way, e].wait_recv()
            own = own + rs_in[way, e, 3].astype(F32)
        sums_ref[e] = own.astype(BF)
    collected = jnp.concatenate(
        [sums_ref[:, :, j * 512 : (j + 1) * 512].reshape(64, 512) for j in range(4)], axis=0
    )
    order = lax.broadcasted_iota(jnp.int32, (256, 256), 1)
    order = ((order // 2) % 16) * 16 + (order // 64) * 4 + ((order // 32) % 2) * 2 + order % 2
    repack = chosen(lax.broadcasted_iota(jnp.int32, (256, 256), 0) == order)
    ret[...] = (
        jnp.dot(repack, collected, preferred_element_type=F32).astype(BF).reshape(16, 16, 512)
    )
    moves += exchange(ret, back, back_send, back_recv)
    returned = back[...].reshape(256, 512)
    result = mixed_ref[...]
    spots = lax.broadcasted_iota(jnp.int32, (96, 256), 1)
    for k in (0, 1):
        select = chosen(spots == spots_ref[:, k : k + 1])
        picked = jnp.dot(select, returned, preferred_element_type=F32)
        picked = jnp.concatenate([picked[j * 24 : (j + 1) * 24] for j in range(4)], axis=1)
        result = result + share_ref[:, k : k + 1] * picked
    out_ref[...] = result.astype(BF)
    for copy in copies + moves:
        copy.wait_send()
    ends = [(ring_send.at[k], size) for k, size in ring]
    ends += [(flip_send.at[k], HALF) for k in range(15)]
    for sem, size in ends:
        pltpu.make_async_remote_copy(
            src_ref=buf.at[0, pl.ds(0, size)], dst_ref=buf.at[0, pl.ds(0, size)],
            send_sem=sem, recv_sem=flip_recv.at[0], device_id=partner, device_id_type=MESH,
        ).wait_send()
    for copy in sent + [weights_over, heads_over]:
        copy.wait_send()


def layer(operands, weights, scale_one, scale_two):
    vmem = pl.BlockSpec(memory_space=pltpu.VMEM)
    hbm = pl.BlockSpec(memory_space=pl.ANY)
    dma = pltpu.SemaphoreType.DMA
    return pl.pallas_call(
        functools.partial(layer_kernel, scale_one=scale_one, scale_two=scale_two),
        out_shape=jax.ShapeDtypeStruct((24, 2048), BF),
        in_specs=[vmem] * len(operands) + [hbm] * len(weights),
        out_specs=vmem,
        scratch_shapes=[
            pltpu.VMEM((384, 384), BF),
            pltpu.VMEM((256, 512), BF),
            pltpu.VMEM((512, 384), BF),
            pltpu.VMEM((15, 416, 512), BF),
            pltpu.VMEM((128, 384), BF),
            pltpu.VMEM((256, 384), BF),
            pltpu.VMEM((384, 384), BF),
            pltpu.VMEM((384, 384), F32),
            pltpu.VMEM((2, 384, 128), F32),
            pltpu.VMEM((256, 2048), BF),
            pltpu.VMEM((2, 192, 384), BF),
            pltpu.VMEM((192, 384), BF),
            pltpu.VMEM((8, 24, 2048), F32),
            pltpu.VMEM((2, 24, 1024), BF),
            pltpu.VMEM((2, 24, 1024), BF),
            pltpu.VMEM((2, 3, 24, 2048), BF),
            pltpu.VMEM((2, 3, 24, 2048), BF),
            pltpu.VMEM((24, 2048), F32),
            pltpu.VMEM((16, 16, 512), BF),
            pltpu.VMEM((16, 16, 512), BF),
            pltpu.VMEM((2, 32, 2048), BF),
            pltpu.VMEM((2, 16, 32, 2048), BF),
            pltpu.VMEM((2, 2048, 256), BF),
            pltpu.VMEM((2, 2048, 256), BF),
            pltpu.VMEM((2, 256, 2048), BF),
            pltpu.VMEM((2, 16, 32, 2048), BF),
            pltpu.VMEM((2, 8, 32, 2048), BF),
            pltpu.VMEM((2, 2, 4, 32, 2048), BF),
            pltpu.VMEM((2, 2, 4, 32, 2048), BF),
            pltpu.VMEM((2, 32, 2048), BF),
            pltpu.VMEM((16, 16, 512), BF),
            pltpu.VMEM((16, 16, 512), BF),
            dma((20,)),
            dma((15, 2)),
            dma((15,)),
            dma((15,)),
            dma((2,)),
            dma((2,)),
            dma((2, 4)),
            dma((2, 4)),
            dma((15,)),
            dma((15,)),
            dma((3,)),
            dma((2, 4, 2)),
            dma((2, 4, 2)),
            dma((8, 2)),
            dma((8, 2)),
            dma((8, 2)),
            dma((8, 2)),
            dma((2, 2, 4)),
            dma((2, 2, 4)),
            dma((15,)),
            dma((15,)),
        ],
        compiler_params=pltpu.CompilerParams(
            collective_id=0, has_side_effects=True, vmem_limit_bytes=60 * 1024 * 1024
        ),
        name="layer",
    )(*operands, *weights)


def angle_tables(places, rope_width):
    frequencies = rope_base ** (-jnp.arange(0, rope_width, 2, dtype=jnp.float32) / rope_width)
    angles = places[:, None] * frequencies[None, :]
    return (jnp.cos(angles), jnp.sin(angles))


def rope_turn(values, cosine, sine_table):
    half_size = values.shape[-1] // 2
    first_half = values[..., :half_size]
    second = values[..., half_size:]
    return jnp.concatenate(
        [first_half * cosine - second * sine_table, second * cosine + first_half * sine_table],
        axis=-1,
    )


def rms_scale(values, gain_vector):
    values = values.astype(jnp.float32)
    inverse = lax.rsqrt(jnp.mean(values * values, axis=-1, keepdims=True) + epsilon)
    return values * inverse * gain_vector


def local(
    residual,
    queries,
    query_rope,
    latent,
    key_rope,
    latent_gain,
    key_weight,
    value_weight,
    out_weight,
    norm_gain,
    routes,
    group_gate,
    expert_share,
    gate_weight,
    up_weight,
    down_weight,
):
    local_tokens = queries.shape[0]
    pair_dev = queries.shape[1]
    tp_count = lax.axis_size(TP)
    row_count = local_tokens // tp_count
    rope_width = key_rope.shape[1]
    first_place = lax.axis_index(SP) * local_tokens
    places = (first_place + jnp.arange(local_tokens, dtype=jnp.int32)).astype(jnp.float32)
    cosine, sine_table = angle_tables(places, rope_width)
    rotated_key = rope_turn(key_rope.astype(jnp.float32), cosine, sine_table).astype(jnp.bfloat16)
    turned = rope_turn(
        query_rope.astype(jnp.float32).reshape(local_tokens, pair_dev, 2, rope_width),
        cosine[:, None, None, :],
        sine_table[:, None, None, :],
    ).astype(jnp.bfloat16)
    compressed = rms_scale(latent, latent_gain).astype(BF)
    scale_one = (DK_A + rope_width) ** (-0.5)
    scale_two = (queries.shape[2] - DK_A + rope_width) ** (-0.5)
    own = jnp.concatenate(
        [jnp.pad(rotated_key.T, ((0, 0), (0, 128))), compressed], axis=0
    )
    flat = queries[:, 0]
    own_routes = lax.dynamic_slice_in_dim(routes, lax.axis_index(TP) * row_count, row_count, 0)
    choices = own_routes.reshape(-1)
    order = jnp.arange(choices.shape[0], dtype=jnp.int32)
    same = (choices[:, None] == choices[None, :]) & (order[:, None] > order[None, :])
    slots = (choices * 2 + jnp.sum(same.astype(jnp.int32), axis=1)).reshape(row_count, 2)
    spots = (slots // 4) * 16 + slots % 4
    quarters = jnp.arange(4, dtype=jnp.int32)
    spots = (spots[None] + 4 * quarters[:, None, None]).reshape(4 * row_count, 2)
    route_weight = group_gate[:, None] * expert_share / jnp.sum(expert_share, axis=1, keepdims=True)
    operands = (
        flat,
        turned.reshape(local_tokens, 2 * rope_width),
        own,
        key_weight[:, 0],
        value_weight[:, 0],
        out_weight[0],
        residual,
        norm_gain[None],
        jnp.tile(slots.T, (1, 4)),
        spots,
        route_weight,
    )
    return layer(operands, (gate_weight, up_weight, down_weight), scale_one, scale_two)


def solution(mesh):
    finer = Mesh(mesh.devices.reshape(4, 4, 8, 2), ("y", "x", "z", "c"))
    placed = (
        P(SP_TP, None),
        P(SP, TP, None),
        P(SP, TP, None),
        P(SP, None),
        P(SP, None),
        P(),
        P(None, TP, None),
        P(None, TP, None),
        P(TP, None, None),
        P(),
        P(SP, None),
        P(SP_TP),
        P(SP_TP, None),
        P(SP, None, TP),
        P(SP, None, TP),
        P(SP, TP, None),
    )
    return jax.shard_map(
        local, mesh=finer, in_specs=placed, out_specs=P(SP_TP, None), check_vma=False
    )
```

```python
import functools

import jax
import jax.numpy as jnp
import numpy as np
from jax import lax
from jax.experimental import pallas as pl
from jax.experimental.pallas import tpu as pltpu
from jax.sharding import Mesh
from jax.sharding import PartitionSpec as P

DK_A = 64
DV_A = 64
SP = ("y", "x")
TP = ("z", "c")
SP_TP = ("y", "x", "z", "c")
MESH = pl.DeviceIdType.MESH
LOG2E = 1.4426950408889634
BF = jnp.bfloat16
F32 = jnp.float32

rope_base = 10000.0
epsilon = 1e-06
floor_score = -1e30

ORDER = (
    (0, 0),
    (0, 1), (0, 3), (1, 0), (3, 0),
    (0, 2), (2, 0),
    (1, 1), (1, 3), (3, 1), (3, 3),
    (1, 2), (3, 2), (2, 1), (2, 3),
    (2, 2),
)
SLOT = {place: k for k, place in enumerate(ORDER)}
HALF = 208
PART = 112


def place():
    return tuple(lax.axis_index(name) for name in ("y", "x", "z", "c"))


def meet(devices):
    barrier = pltpu.get_barrier_semaphore()
    for device in devices:
        pl.semaphore_signal(barrier, inc=1, device_id=device, device_id_type=MESH)
    pl.semaphore_wait(barrier, len(devices))


DZ = (0, -1, 1, -2, 2, -3, 3, 4)
BASE = {dz: 2 * k for k, dz in enumerate(DZ)}


def spread_place(column):
    return column + jnp.where(column >= DK_A, 64, 0)


def chosen(condition):
    return jnp.where(condition, 1.0, 0.0).astype(BF)


def layer_kernel(
    q_ref, q_rope_ref, latent_ref, key_rope_ref, latent_gain_ref, pace_ref,
    wk_ref, wv_ref, ow_ref, residual_ref, gain_ref,
    routes_ref, group_ref, share_ref, gate_hbm, up_hbm, down_hbm, out_ref,
    own_ref, sel, qx, wkt, buf, kta, ktb, vx, acc, top, weight_sum, owp, attx, attr, part,
    step_out, step_in, mixed_ref, disp, arr, rows_ref,
    held, gate, up, down, made, given, rs_out, rs_in, sums_ref, ret, back,
    ring_send, ring_recv, flip_send, flip_recv, misc_send, misc_recv, head_send, head_recv,
    disp_send, disp_recv, load_sem, z_send, z_recv, swap_send, swap_recv,
    give_send, give_recv, rs_send, rs_recv, back_send, back_recv,
    *, scale_one, scale_two,
):
    y, x, z, c = place()
    partner = (y, x, z, 1 - c)

    def along_a(step):
        return ((y + c * step + 4) % 4, (x + (1 - c) * step + 4) % 4, z, c)

    def along_b(step):
        return ((y + (1 - c) * step + 4) % 4, (x + c * step + 4) % 4, z, c)

    def along_z(step):
        return (y, x, (z + step + 8) % 8, c)

    def slot(da, db):
        first = SLOT[(db % 4, da % 4)]
        second = SLOT[(da % 4, db % 4)]
        return first if first == second else first + c * (second - first)

    me = y * 4 + x
    peers = [
        (dy, dx, ((y + dy) % 4, (x + dx) % 4, z, c))
        for dy in range(4) for dx in range(4) if dy or dx
    ]
    loads = [
        pltpu.make_async_copy(src, dst, load_sem.at[k])
        for k, (src, dst) in enumerate(((gate_hbm, gate), (up_hbm, up), (down_hbm, down)))
    ]
    for load in loads:
        load.start()
    angles = (me * 384 + lax.broadcasted_iota(jnp.int32, (16, 384), 1)).astype(F32)
    angles = angles * pace_ref[...]
    cosine = jnp.cos(angles)
    sine = jnp.sin(angles)

    def turn(pair):
        first, second = pair[0:16], pair[16:32]
        return [first * cosine - second * sine, second * cosine + first * sine]

    keys = key_rope_ref[...].astype(F32)
    own_ref[0:32, 0:384] = jnp.concatenate(turn(keys), axis=0).astype(BF)
    own_ref[0:32, 384:512] = jnp.zeros((32, 128), BF)
    latent = latent_ref[...].astype(F32)
    inverse = lax.rsqrt(jnp.mean(latent * latent, axis=1, keepdims=True) + epsilon)
    own_ref[32:416] = (latent * inverse * latent_gain_ref[...]).astype(BF)
    meet([partner, along_z(1), along_z(-1)] + [peer[2] for peer in peers])
    start_row = c * HALF
    other_row = (1 - c) * HALF
    counts = {"ring": 0}
    ring = []

    def piece(k, first, size):
        return buf.at[k - 1, pl.ds(pl.multiple_of(start_row + first, 16), size)]

    spans = {None: (0, HALF), 0: (0, PART), 1: (PART, HALF - PART)}

    def send(source, target, device, which=None):
        first, size = spans[which]
        if source is None:
            src = own_ref.at[pl.ds(pl.multiple_of(start_row + first, 16), size)]
        else:
            src = piece(source, first, size)
        copy = pltpu.make_async_remote_copy(
            src_ref=src,
            dst_ref=piece(target, first, size),
            send_sem=ring_send.at[counts["ring"]],
            recv_sem=ring_recv.at[target - 1, which or 0],
            device_id=device,
            device_id_type=MESH,
        )
        ring.append((counts["ring"], size))
        counts["ring"] += 1
        copy.start()

    def arrived(k, which=None):
        first, size = spans[which]
        pltpu.make_async_remote_copy(
            src_ref=piece(k, first, size),
            dst_ref=piece(k, first, size),
            send_sem=ring_send.at[0],
            recv_sem=ring_recv.at[k - 1, which or 0],
            device_id=partner,
            device_id_type=MESH,
        ).wait_recv()

    def flip(k):
        copy = pltpu.make_async_remote_copy(
            src_ref=piece(k, 0, HALF),
            dst_ref=piece(k, 0, HALF),
            send_sem=flip_send.at[k - 1],
            recv_sem=flip_recv.at[k - 1],
            device_id=partner,
            device_id_type=MESH,
        )
        copy.start()

    def flipped(k):
        there = buf.at[k - 1, pl.ds(pl.multiple_of(other_row, 16), HALF)]
        pltpu.make_async_remote_copy(
            src_ref=there, dst_ref=there,
            send_sem=flip_send.at[0], recv_sem=flip_recv.at[k - 1],
            device_id=partner, device_id_type=MESH,
        ).wait_recv()

    for sign in (1, -1):
        send(None, slot(-sign, 0), along_a(sign))
    weights_over = pltpu.make_async_remote_copy(
        src_ref=ow_ref, dst_ref=owp, send_sem=misc_send.at[0], recv_sem=misc_recv.at[0],
        device_id=partner, device_id_type=MESH,
    )
    weights_over.start()

    queries = q_rope_ref[...].astype(F32)
    turned = jnp.concatenate(turn(queries[0:32]) + turn(queries[32:64]), axis=0).astype(BF)
    spread = chosen(
        lax.broadcasted_iota(jnp.int32, (256, 384), 1)
        == spread_place(lax.broadcasted_iota(jnp.int32, (256, 384), 0))
    )
    turns = lax.broadcasted_iota(jnp.int32, (64, 384), 0)
    turns = chosen(
        lax.broadcasted_iota(jnp.int32, (64, 384), 1)
        == turns + 64 + jnp.where(turns >= 32, 224, 0)
    )
    qx[...] = (
        jnp.dot(q_ref[...], spread, preferred_element_type=F32)
        + lax.dot_general(
            turned, turns, (((0,), (0,)), ((), ())), preferred_element_type=F32
        )
    ).astype(BF)
    unit = chosen(
        lax.broadcasted_iota(jnp.int32, (256, 256), 0)
        == lax.broadcasted_iota(jnp.int32, (256, 256), 1)
    )
    wkt[...] = lax.dot_general(
        unit, wk_ref[...], (((1,), (1,)), ((), ())), preferred_element_type=F32
    ).astype(BF)
    tokens = lax.broadcasted_iota(jnp.int32, (24, 384), 0) + (z * 2 + c) * 24
    mine = chosen(lax.broadcasted_iota(jnp.int32, (24, 384), 1) == tokens)
    routes = lax.dot_general(
        mine, routes_ref[...].astype(F32).astype(BF), (((1,), (1,)), ((), ())),
        preferred_element_type=F32,
    )
    experts = lax.broadcasted_iota(jnp.int32, (24, 32), 1).astype(F32)
    named = [routes[:, k : k + 1] == experts for k in (0, 1)]
    earlier = chosen(
        lax.broadcasted_iota(jnp.int32, (24, 24), 0) > lax.broadcasted_iota(jnp.int32, (24, 24), 1)
    )
    before = jnp.dot(earlier, chosen(named[0] | named[1]), preferred_element_type=F32)
    packed = lax.broadcasted_iota(jnp.int32, (96, 256), 1).astype(F32)
    for k in (0, 1):
        rank = jnp.sum(jnp.where(named[k], before, 0.0), axis=1, keepdims=True)
        expert = routes[:, k : k + 1]
        spot = jnp.floor(expert * 0.5) * 12.0 + expert * 2.0 + rank
        spots = jnp.concatenate([spot + 4.0 * j for j in range(4)], axis=0)
        sel[k] = chosen(packed == spots)
    kta[96:128] = jnp.zeros((32, 384), BF)
    ktb[224:256] = jnp.zeros((32, 384), BF)
    heads = (
        (slice(0, 128), kta, 0, scale_one * LOG2E),
        (slice(128, 384), ktb, 1, scale_two * LOG2E),
    )

    def block(ref, first):
        rope = ref[0:32, 0:384]
        lat = ref[32:416, :]
        keys = lax.dot_general(
            wkt[...], lat, (((1,), (1,)), ((), ())), preferred_element_type=F32
        ).astype(BF)
        kta[0:64] = keys[0:64]
        kta[64:96] = rope
        ktb[0:192] = keys[64:256]
        ktb[192:224] = rope
        vx[...] = jnp.dot(lat, wv_ref[...], preferred_element_type=F32).astype(BF)
        for cols, keys_ref, h, factor in heads:
            scores = jnp.dot(qx[:, cols], keys_ref[...], preferred_element_type=F32)
            if first:
                rows = lax.broadcasted_iota(jnp.int32, (384, 384), 0)
                places = lax.broadcasted_iota(jnp.int32, (384, 384), 1)
                scores = jnp.where(rows >= places, scores, floor_score)
            peak = jnp.max(scores, axis=1, keepdims=True)
            width = (cols.stop - cols.start) // 128
            if first:
                new = jnp.broadcast_to(peak, (384, 128))
            else:
                old = top[h]
                new = jnp.maximum(old, peak)
            top[h] = new
            weights = jnp.exp2((scores - jnp.concatenate([new] * 3, axis=1)) * factor)
            sums = weights[:, 0:128] + weights[:, 128:256] + weights[:, 256:384]
            update = jnp.dot(weights.astype(BF), vx[:, 0 : 128 * width], preferred_element_type=F32)
            if first:
                weight_sum[h] = sums
                acc[:, cols] = update
            else:
                shrink = jnp.exp2((old - new) * factor)
                weight_sum[h] = weight_sum[h] * shrink + sums
                acc[:, cols] = acc[:, cols] * jnp.concatenate([shrink] * width, axis=1) + update

    for sign in (1, -1):
        send(None, slot(0, -sign), along_b(sign))
    block(own_ref, True)

    def step(i, carry):
        @pl.when(i == 1)
        def _():
            near = []
            for sign in (1, -1):
                k = slot(-sign, 0)
                arrived(k)
                flip(k)
                send(k, slot(-2 * sign, 0), along_a(sign), 0 if sign == 1 else 1)
                near.append(k)
                k = slot(0, -sign)
                arrived(k)
                flip(k)
                send(k, slot(0, -2 * sign), along_b(sign), 0 if sign == 1 else 1)
            for sign, k in zip((1, -1), near):
                send(k, slot(-sign, -1), along_b(1))
                send(k, slot(-sign, 1), along_b(-1))

        @pl.when(i == 4)
        def _():
            k = slot(2, 0)
            arrived(k, 0)
            arrived(k, 1)
            flip(k)
            send(k, slot(2, -1), along_b(1))
            send(k, slot(2, 1), along_b(-1))
            k = slot(0, 2)
            arrived(k, 0)
            arrived(k, 1)
            flip(k)

        @pl.when(i == 7)
        def _():
            for da in (-1, 1):
                for sign in (1, -1):
                    k = slot(da, -sign)
                    arrived(k)
                    flip(k)
                    send(k, slot(da, -2 * sign), along_b(sign), 0 if sign == 1 else 1)

        @pl.when(i == 8)
        def _():
            for sign in (1, -1):
                k = slot(2, -sign)
                arrived(k)
                flip(k)
                send(k, slot(2, -2 * sign), along_b(sign), 0 if sign == 1 else 1)

        @pl.when(i == 10)
        def _():
            for da in (-1, 1):
                k = slot(da, 2)
                arrived(k, 0)
                arrived(k, 1)
                flip(k)

        @pl.when(i == 11)
        def _():
            k = slot(2, 2)
            arrived(k, 0)
            arrived(k, 1)
            flip(k)

        flipped(i)
        dy = 0
        dx = 0
        for k in range(1, 16):
            dy = jnp.where(i == k, ORDER[k][0], dy)
            dx = jnp.where(i == k, ORDER[k][1], dx)
        theirs = ((y + dy) % 4) * 4 + (x + dx) % 4

        @pl.when(theirs < me)
        def _():
            block(buf.at[i - 1], False)

        return carry

    lax.fori_loop(1, 16, step, 0)

    total = acc[...]
    part_a = total[:, 0:128] / jnp.sum(weight_sum[0], axis=1, keepdims=True)
    part_b = total[:, 128:384] / jnp.sum(weight_sum[1], axis=1, keepdims=True)
    low = lax.broadcasted_iota(jnp.int32, (384, 128), 1) < DV_A
    both = jnp.concatenate([jnp.where(low, part_a, part_b[:, 0:128]), part_b[:, 128:256]], axis=1)
    for side in (0, 1):
        attx[side] = jnp.concatenate(
            [both[(2 * k + side) * 24 : (2 * k + side + 1) * 24] for k in range(8)], axis=0
        ).astype(BF)
    heads_over = pltpu.make_async_remote_copy(
        src_ref=attx.at[1 - c], dst_ref=attr, send_sem=misc_send.at[1], recv_sem=misc_recv.at[1],
        device_id=partner, device_id_type=MESH,
    )
    heads_over.start()
    weights_over.wait_recv()
    partial = jnp.dot(attx[c], ow_ref[...], preferred_element_type=F32)
    heads_over.wait_recv()
    partial = partial + jnp.dot(attr[...], owp[...], preferred_element_type=F32)
    part[...] = partial.reshape(8, 24, 2048)

    sent = []
    chains = {}

    def pass_on(way, side, hop, value):
        step_out[way, side, hop] = value.astype(BF)
        copy = pltpu.make_async_remote_copy(
            src_ref=step_out.at[way, side, hop], dst_ref=step_in.at[way, side, hop],
            send_sem=head_send.at[way, side, hop], recv_sem=head_recv.at[way, side, hop],
            device_id=along_z(1 if way == 0 else -1), device_id_type=MESH,
        )
        copy.start()
        sent.append(copy)
        chains[way, side] = copy

    def head_part(dz, side):
        return part[(z + dz + 8) % 8, :, side * 512 : (side + 1) * 512]

    far = ((0, 0), (1, 2), (0, 1), (1, 3))
    near = ((0, 2), (1, 0), (0, 3), (1, 1))
    for way, side in far:
        pass_on(way, side, 0, head_part(4, side))
    for way, side in near:
        pass_on(way, side, 1, head_part(3 if way == 0 else -3, side))
    for hop in (1, 2, 3):
        for way, side in far:
            chains[way, side].wait_recv()
            dz = (4 - hop) * (1 if way == 0 else -1)
            got = step_in[way, side, hop - 1].astype(F32)
            pass_on(way, side, hop, head_part(dz, side) + got)
        if hop < 3:
            for way, side in near:
                chains[way, side].wait_recv()
                dz = (3 - hop) * (1 if way == 0 else -1)
                got = step_in[way, side, hop].astype(F32)
                pass_on(way, side, hop + 1, head_part(dz, side) + got)
    for chain in chains.values():
        chain.wait_recv()
    arrived_sums = [
        jnp.concatenate([step_in[way, side, 3] for side in range(4)], axis=1).astype(F32)
        for way in (0, 1)
    ]
    mixed = residual_ref[...].astype(F32) + part[z]
    mixed = mixed + arrived_sums[0] + arrived_sums[1]
    mixed_ref[...] = mixed
    inverse = lax.rsqrt(jnp.mean(mixed * mixed, axis=1, keepdims=True) + epsilon)
    normed = mixed * inverse * gain_ref[...]
    stack = jnp.concatenate([normed[:, j * 512 : (j + 1) * 512] for j in range(4)], axis=0)
    outgoing = lax.dot_general(
        sel[0] + sel[1], stack.astype(BF), (((0,), (0,)), ((), ())), preferred_element_type=F32
    ).astype(BF)
    disp[...] = outgoing.reshape(16, 16, 512)

    def exchange(source, target, send_sem, recv_sem):
        target[me] = source[me]
        moves = []
        for dy, dx, peer in peers:
            there = peer[0] * 4 + peer[1]
            k = dy * 4 + dx - 1
            copy = pltpu.make_async_remote_copy(
                src_ref=source.at[there], dst_ref=target.at[me],
                send_sem=send_sem.at[k], recv_sem=recv_sem.at[k],
                device_id=peer, device_id_type=MESH,
            )
            copy.start()
            moves.append(copy)
        for copy in moves:
            copy.wait_recv()
        return moves

    moves = exchange(disp, arr, disp_send, disp_recv)
    order = lax.broadcasted_iota(jnp.int32, (256, 256), 0)
    order = ((order // 2) % 16) * 16 + (order // 64) * 4 + ((order // 32) % 2) * 2 + order % 2
    unpack = chosen(lax.broadcasted_iota(jnp.int32, (256, 256), 1) == order)
    arrived_rows = jnp.dot(
        unpack, arr[...].reshape(256, 512), preferred_element_type=F32
    ).astype(BF)
    for j in range(4):
        piece_rows = arrived_rows[j * 64 : (j + 1) * 64].reshape(2, 32, 512)
        rows_ref[:, :, j * 512 : (j + 1) * 512] = piece_rows

    copies = []

    def remote(src, dst, send_sem, recv_sem, device):
        copy = pltpu.make_async_remote_copy(
            src_ref=src, dst_ref=dst, send_sem=send_sem, recv_sem=recv_sem,
            device_id=device, device_id_type=MESH,
        )
        copy.start()
        copies.append(copy)
        return copy

    hops = {}
    flips = {}
    for e in (0, 1):
        for way, sign in ((0, 1), (1, -1)):
            hops[way, 1, e] = remote(
                rows_ref.at[e], held.at[e, BASE[-sign] + c],
                z_send.at[way, 0, e], z_recv.at[way, 0, e], along_z(sign),
            )
        flips[0, e] = remote(
            rows_ref.at[e], held.at[e, c], swap_send.at[0, e], swap_recv.at[0, e], partner
        )
        held[e, c] = rows_ref[e]

    def compute(first, count, dzs):
        for e in (0, 1):
            rows = held[e, first : first + count].reshape(count * 32, 2048)
            inner = jnp.dot(rows, gate[e], preferred_element_type=F32)
            inner = inner / (1.0 + jnp.exp(-inner))
            inner = inner * jnp.dot(rows, up[e], preferred_element_type=F32)
            result = jnp.dot(inner.astype(BF), down[e], preferred_element_type=F32)
            made[e, first : first + count] = result.astype(BF).reshape(count, 32, 2048)
            for dz in dzs:
                k = BASE[dz] // 2
                gives[dz, e] = remote(
                    made.at[e, BASE[dz] + 1 - c], given.at[e, k],
                    give_send.at[k, e], give_recv.at[k, e], partner,
                )

    gives = {}

    def chip_sum(dz, e):
        if (dz, e) in gives:
            gives.pop((dz, e)).wait_recv()
        return made[e, BASE[dz] + c].astype(F32) + given[e, BASE[dz] // 2].astype(F32)

    for load in loads:
        load.wait()
    for e in (0, 1):
        flips[0, e].wait_recv()
    compute(0, 2, (0,))
    for dist in (1, 2, 3):
        for e in (0, 1):
            for way, sign in ((0, 1), (1, -1)):
                hops[way, dist, e].wait_recv()
                dz = -sign * dist
                spot = held.at[e, BASE[dz] + c]
                k = BASE[dz] // 2
                if dist < 3:
                    target = held.at[e, BASE[dz - sign] + c]
                elif way == e:
                    target = held.at[e, BASE[4] + c]
                else:
                    target = None
                if target is not None:
                    hops[way, dist + 1, e] = remote(
                        spot, target, z_send.at[way, dist, e], z_recv.at[way, dist, e],
                        along_z(sign),
                    )
                flips[k, e] = remote(
                    spot, spot, swap_send.at[k, e], swap_recv.at[k, e], partner
                )
        for e in (0, 1):
            for dz in (-dist, dist):
                flips[BASE[dz] // 2, e].wait_recv()
        compute(4 * dist - 2, 4, (-dist, dist))

    sums = {}

    def push(way, e, hop, value):
        sign = 1 if way == 0 else -1
        rs_out[way, e, hop] = value.astype(BF)
        sums[way, e] = remote(
            rs_out.at[way, e, hop], rs_in.at[way, e, hop],
            rs_send.at[way, e, hop], rs_recv.at[way, e, hop], along_z(sign),
        )

    push(0, 1, 1, chip_sum(3, 1))
    push(1, 0, 1, chip_sum(-3, 0))
    for e in (0, 1):
        hops[e, 4, e].wait_recv()
        spot = held.at[e, BASE[4] + c]
        flips[7, e] = remote(spot, spot, swap_send.at[7, e], swap_recv.at[7, e], partner)
    for e in (0, 1):
        flips[7, e].wait_recv()
    compute(14, 2, (4,))
    push(0, 0, 0, chip_sum(4, 0))
    push(1, 1, 0, chip_sum(4, 1))
    for hop in (1, 2, 3):
        if hop < 3:
            for way, e in ((0, 1), (1, 0)):
                sums[way, e].wait_recv()
                dz = (3 - hop) * (1 if way == 0 else -1)
                push(way, e, hop + 1, chip_sum(dz, e) + rs_in[way, e, hop].astype(F32))
        for way, e in ((0, 0), (1, 1)):
            sums[way, e].wait_recv()
            dz = (4 - hop) * (1 if way == 0 else -1)
            push(way, e, hop, chip_sum(dz, e) + rs_in[way, e, hop - 1].astype(F32))
    for e in (0, 1):
        own = chip_sum(0, e)
        for way in (0, 1):
            sums[way, e].wait_recv()
            own = own + rs_in[way, e, 3].astype(F32)
        sums_ref[e] = own.astype(BF)
    collected = jnp.concatenate(
        [sums_ref[:, :, j * 512 : (j + 1) * 512].reshape(64, 512) for j in range(4)], axis=0
    )
    order = lax.broadcasted_iota(jnp.int32, (256, 256), 1)
    order = ((order // 2) % 16) * 16 + (order // 64) * 4 + ((order // 32) % 2) * 2 + order % 2
    repack = chosen(lax.broadcasted_iota(jnp.int32, (256, 256), 0) == order)
    ret[...] = (
        jnp.dot(repack, collected, preferred_element_type=F32).astype(BF).reshape(16, 16, 512)
    )
    moves += exchange(ret, back, back_send, back_recv)
    returned = back[...].reshape(256, 512)
    result = mixed_ref[...]
    eye = lax.broadcasted_iota(jnp.int32, (24, 24), 0)
    eye = eye == lax.broadcasted_iota(jnp.int32, (24, 24), 1)
    groups = jnp.sum(jnp.where(eye, group_ref[...], 0.0), axis=1, keepdims=True)
    shares = [
        jnp.sum(jnp.where(eye, share_ref[k : k + 1], 0.0), axis=1, keepdims=True) for k in (0, 1)
    ]
    for k in (0, 1):
        picked = jnp.dot(sel[k], returned, preferred_element_type=F32)
        picked = jnp.concatenate([picked[j * 24 : (j + 1) * 24] for j in range(4)], axis=1)
        result = result + groups * shares[k] / (shares[0] + shares[1]) * picked
    out_ref[...] = result
    for copy in copies + moves:
        copy.wait_send()
    ends = [(ring_send.at[k], size) for k, size in ring]
    ends += [(flip_send.at[k], HALF) for k in range(15)]
    for sem, size in ends:
        pltpu.make_async_remote_copy(
            src_ref=buf.at[0, pl.ds(0, size)], dst_ref=buf.at[0, pl.ds(0, size)],
            send_sem=sem, recv_sem=flip_recv.at[0], device_id=partner, device_id_type=MESH,
        ).wait_send()
    for copy in sent + [weights_over, heads_over]:
        copy.wait_send()


def layer(operands, weights, scale_one, scale_two):
    vmem = pl.BlockSpec(memory_space=pltpu.VMEM)
    hbm = pl.BlockSpec(memory_space=pl.ANY)
    dma = pltpu.SemaphoreType.DMA
    return pl.pallas_call(
        functools.partial(layer_kernel, scale_one=scale_one, scale_two=scale_two),
        out_shape=jax.ShapeDtypeStruct((24, 2048), F32),
        in_specs=[vmem] * len(operands) + [hbm] * len(weights),
        out_specs=vmem,
        scratch_shapes=[
            pltpu.VMEM((416, 512), BF),
            pltpu.VMEM((2, 96, 256), BF),
            pltpu.VMEM((384, 384), BF),
            pltpu.VMEM((256, 512), BF),
            pltpu.VMEM((15, 416, 512), BF),
            pltpu.VMEM((128, 384), BF),
            pltpu.VMEM((256, 384), BF),
            pltpu.VMEM((384, 256), BF),
            pltpu.VMEM((384, 384), F32),
            pltpu.VMEM((2, 384, 128), F32),
            pltpu.VMEM((2, 384, 128), F32),
            pltpu.VMEM((256, 2048), BF),
            pltpu.VMEM((2, 192, 256), BF),
            pltpu.VMEM((192, 256), BF),
            pltpu.VMEM((8, 24, 2048), F32),
            pltpu.VMEM((2, 4, 4, 24, 512), BF),
            pltpu.VMEM((2, 4, 4, 24, 512), BF),
            pltpu.VMEM((24, 2048), F32),
            pltpu.VMEM((16, 16, 512), BF),
            pltpu.VMEM((16, 16, 512), BF),
            pltpu.VMEM((2, 32, 2048), BF),
            pltpu.VMEM((2, 16, 32, 2048), BF),
            pltpu.VMEM((2, 2048, 256), BF),
            pltpu.VMEM((2, 2048, 256), BF),
            pltpu.VMEM((2, 256, 2048), BF),
            pltpu.VMEM((2, 16, 32, 2048), BF),
            pltpu.VMEM((2, 8, 32, 2048), BF),
            pltpu.VMEM((2, 2, 4, 32, 2048), BF),
            pltpu.VMEM((2, 2, 4, 32, 2048), BF),
            pltpu.VMEM((2, 32, 2048), BF),
            pltpu.VMEM((16, 16, 512), BF),
            pltpu.VMEM((16, 16, 512), BF),
            dma((20,)),
            dma((15, 2)),
            dma((15,)),
            dma((15,)),
            dma((2,)),
            dma((2,)),
            dma((2, 4, 4)),
            dma((2, 4, 4)),
            dma((15,)),
            dma((15,)),
            dma((3,)),
            dma((2, 4, 2)),
            dma((2, 4, 2)),
            dma((8, 2)),
            dma((8, 2)),
            dma((8, 2)),
            dma((8, 2)),
            dma((2, 2, 4)),
            dma((2, 2, 4)),
            dma((15,)),
            dma((15,)),
        ],
        compiler_params=pltpu.CompilerParams(
            collective_id=0, has_side_effects=True, vmem_limit_bytes=60 * 1024 * 1024
        ),
        name="layer",
    )(*operands, *weights)


def local(
    residual,
    queries,
    query_rope,
    latent,
    key_rope,
    latent_gain,
    key_weight,
    value_weight,
    out_weight,
    norm_gain,
    routes,
    group_gate,
    expert_share,
    gate_weight,
    up_weight,
    down_weight,
):
    rope_width = key_rope.shape[1]
    scale_one = (DK_A + rope_width) ** (-0.5)
    scale_two = (queries.shape[2] - DK_A + rope_width) ** (-0.5)
    pace = np.float64(rope_base) ** (-np.arange(0, rope_width, 2) / rope_width)
    operands = (
        queries[:, 0],
        query_rope[:, 0].T,
        latent,
        key_rope.T,
        latent_gain[None],
        jnp.asarray(pace[:, None], F32),
        key_weight[:, 0],
        value_weight[:, 0],
        out_weight[0],
        residual,
        norm_gain[None],
        routes.T,
        group_gate[None],
        expert_share.T,
    )
    out = layer(operands, (gate_weight, up_weight, down_weight), scale_one, scale_two)
    return out.astype(BF)


def solution(mesh):
    finer = Mesh(mesh.devices.reshape(4, 4, 8, 2), ("y", "x", "z", "c"))
    placed = (
        P(SP_TP, None),
        P(SP, TP, None),
        P(SP, TP, None),
        P(SP, None),
        P(SP, None),
        P(),
        P(None, TP, None),
        P(None, TP, None),
        P(TP, None, None),
        P(),
        P(SP, None),
        P(SP_TP),
        P(SP_TP, None),
        P(SP, None, TP),
        P(SP, None, TP),
        P(SP, TP, None),
    )
    return jax.shard_map(
        local, mesh=finer, in_specs=placed, out_specs=P(SP_TP, None), check_vma=False
    )
```

```python
import functools

import jax
import jax.numpy as jnp
import numpy as np
from jax import lax
from jax.experimental import pallas as pl
from jax.experimental.pallas import tpu as pltpu
from jax.sharding import Mesh
from jax.sharding import PartitionSpec as P

DK_A = 64
DV_A = 64
SP = ("y", "x")
TP = ("z", "c")
SP_TP = ("y", "x", "z", "c")
MESH = pl.DeviceIdType.MESH
LOG2E = 1.4426950408889634
BF = jnp.bfloat16
F32 = jnp.float32

rope_base = 10000.0
epsilon = 1e-06
floor_score = -1e30

ORDER = (
    (0, 0),
    (0, 1), (0, 3), (1, 0), (3, 0),
    (0, 2), (2, 0),
    (1, 1), (1, 3), (3, 1), (3, 3),
    (1, 2), (3, 2), (2, 1), (2, 3),
    (2, 2),
)
SLOT = {place: k for k, place in enumerate(ORDER)}
HALF = 208
PART = 112


def place():
    return tuple(lax.axis_index(name) for name in ("y", "x", "z", "c"))


def meet(devices):
    barrier = pltpu.get_barrier_semaphore()
    for device in devices:
        pl.semaphore_signal(barrier, inc=1, device_id=device, device_id_type=MESH)
    pl.semaphore_wait(barrier, len(devices))


DZ = (0, -1, 1, -2, 2, -3, 3, 4)
BASE = {dz: 2 * k for k, dz in enumerate(DZ)}


def spread_place(column):
    return column + jnp.where(column >= DK_A, 64, 0)


def chosen(condition):
    return jnp.where(condition, 1.0, 0.0).astype(BF)


def layer_kernel(
    q_ref, q_rope_ref, latent_ref, key_rope_ref, latent_gain_ref, pace_ref,
    wk_ref, wv_ref, ow_ref, residual_ref, gain_ref,
    routes_ref, group_ref, share_ref, gate_hbm, up_hbm, down_hbm, out_ref,
    own_ref, sel, qx, wkt, buf, kta, ktb, vx, acc, top, weight_sum, owp, attx, attr, part,
    step_out, step_in, mixed_ref, disp, arr, rows_ref,
    held, gate, up, down, made, given, rs_out, rs_in, sums_ref, ret, back,
    ring_send, ring_recv, flip_send, flip_recv, misc_send, misc_recv, head_send, head_recv,
    disp_send, disp_recv, load_sem, z_send, z_recv, swap_send, swap_recv,
    give_send, give_recv, rs_send, rs_recv, back_send, back_recv,
    *, scale_one, scale_two,
):
    y, x, z, c = place()
    partner = (y, x, z, 1 - c)

    def along_a(step):
        return ((y + c * step + 4) % 4, (x + (1 - c) * step + 4) % 4, z, c)

    def along_b(step):
        return ((y + (1 - c) * step + 4) % 4, (x + c * step + 4) % 4, z, c)

    def along_z(step):
        return (y, x, (z + step + 8) % 8, c)

    def slot(da, db):
        first = SLOT[(db % 4, da % 4)]
        second = SLOT[(da % 4, db % 4)]
        return first if first == second else first + c * (second - first)

    me = y * 4 + x
    peers = [
        (dy, dx, ((y + dy) % 4, (x + dx) % 4, z, c))
        for dy, dx in sorted(ORDER[1:], key=lambda p: -(min(p[0], 4 - p[0]) + min(p[1], 4 - p[1])))
    ]
    loads = [
        pltpu.make_async_copy(src, dst, load_sem.at[k])
        for k, (src, dst) in enumerate(((gate_hbm, gate), (up_hbm, up), (down_hbm, down)))
    ]
    for load in loads:
        load.start()
    angles = (me * 384 + lax.broadcasted_iota(jnp.int32, (16, 384), 1)).astype(F32)
    angles = angles * pace_ref[...]
    cosine = jnp.cos(angles)
    sine = jnp.sin(angles)

    def turn(pair):
        first, second = pair[0:16], pair[16:32]
        return [first * cosine - second * sine, second * cosine + first * sine]

    keys = key_rope_ref[...].astype(F32)
    own_ref[0:32, 0:384] = jnp.concatenate(turn(keys), axis=0).astype(BF)
    own_ref[0:32, 384:512] = jnp.zeros((32, 128), BF)
    latent = latent_ref[...].astype(F32)
    inverse = lax.rsqrt(jnp.mean(latent * latent, axis=1, keepdims=True) + epsilon)
    own_ref[32:416] = (latent * inverse * latent_gain_ref[...]).astype(BF)
    meet([partner, along_z(1), along_z(-1)] + [peer[2] for peer in peers])
    start_row = c * HALF
    other_row = (1 - c) * HALF
    counts = {"ring": 0}
    ring = []

    def piece(k, first, size):
        return buf.at[k - 1, pl.ds(pl.multiple_of(start_row + first, 16), size)]

    spans = {None: (0, HALF), 0: (0, PART), 1: (PART, HALF - PART)}

    def send(source, target, device, which=None):
        first, size = spans[which]
        if source is None:
            src = own_ref.at[pl.ds(pl.multiple_of(start_row + first, 16), size)]
        else:
            src = piece(source, first, size)
        copy = pltpu.make_async_remote_copy(
            src_ref=src,
            dst_ref=piece(target, first, size),
            send_sem=ring_send.at[counts["ring"]],
            recv_sem=ring_recv.at[target - 1, which or 0],
            device_id=device,
            device_id_type=MESH,
        )
        ring.append((counts["ring"], size))
        counts["ring"] += 1
        copy.start()

    def arrived(k, which=None):
        first, size = spans[which]
        pltpu.make_async_remote_copy(
            src_ref=piece(k, first, size),
            dst_ref=piece(k, first, size),
            send_sem=ring_send.at[0],
            recv_sem=ring_recv.at[k - 1, which or 0],
            device_id=partner,
            device_id_type=MESH,
        ).wait_recv()

    def flip(k):
        copy = pltpu.make_async_remote_copy(
            src_ref=piece(k, 0, HALF),
            dst_ref=piece(k, 0, HALF),
            send_sem=flip_send.at[k - 1],
            recv_sem=flip_recv.at[k - 1],
            device_id=partner,
            device_id_type=MESH,
        )
        copy.start()

    def flipped(k):
        there = buf.at[k - 1, pl.ds(pl.multiple_of(other_row, 16), HALF)]
        pltpu.make_async_remote_copy(
            src_ref=there, dst_ref=there,
            send_sem=flip_send.at[0], recv_sem=flip_recv.at[k - 1],
            device_id=partner, device_id_type=MESH,
        ).wait_recv()

    for sign in (1, -1):
        send(None, slot(-sign, 0), along_a(sign))
    weights_over = pltpu.make_async_remote_copy(
        src_ref=ow_ref, dst_ref=owp, send_sem=misc_send.at[0], recv_sem=misc_recv.at[0],
        device_id=partner, device_id_type=MESH,
    )
    weights_over.start()

    queries = q_rope_ref[...].astype(F32)
    turned = jnp.concatenate(turn(queries[0:32]) + turn(queries[32:64]), axis=0).astype(BF)
    spread = chosen(
        lax.broadcasted_iota(jnp.int32, (256, 384), 1)
        == spread_place(lax.broadcasted_iota(jnp.int32, (256, 384), 0))
    )
    turns = lax.broadcasted_iota(jnp.int32, (64, 384), 0)
    turns = chosen(
        lax.broadcasted_iota(jnp.int32, (64, 384), 1)
        == turns + 64 + jnp.where(turns >= 32, 224, 0)
    )
    qx[...] = (
        jnp.dot(q_ref[...], spread, preferred_element_type=F32)
        + lax.dot_general(
            turned, turns, (((0,), (0,)), ((), ())), preferred_element_type=F32
        )
    ).astype(BF)
    unit = chosen(
        lax.broadcasted_iota(jnp.int32, (256, 256), 0)
        == lax.broadcasted_iota(jnp.int32, (256, 256), 1)
    )
    wkt[...] = lax.dot_general(
        unit, wk_ref[...], (((1,), (1,)), ((), ())), preferred_element_type=F32
    ).astype(BF)
    tokens = lax.broadcasted_iota(jnp.int32, (24, 384), 0) + (z * 2 + c) * 24
    mine = chosen(lax.broadcasted_iota(jnp.int32, (24, 384), 1) == tokens)
    routes = lax.dot_general(
        mine, routes_ref[...].astype(F32).astype(BF), (((1,), (1,)), ((), ())),
        preferred_element_type=F32,
    )
    experts = lax.broadcasted_iota(jnp.int32, (24, 32), 1).astype(F32)
    named = [routes[:, k : k + 1] == experts for k in (0, 1)]
    earlier = chosen(
        lax.broadcasted_iota(jnp.int32, (24, 24), 0) > lax.broadcasted_iota(jnp.int32, (24, 24), 1)
    )
    before = jnp.dot(earlier, chosen(named[0] | named[1]), preferred_element_type=F32)
    packed = lax.broadcasted_iota(jnp.int32, (96, 256), 1).astype(F32)
    for k in (0, 1):
        rank = jnp.sum(jnp.where(named[k], before, 0.0), axis=1, keepdims=True)
        expert = routes[:, k : k + 1]
        spot = jnp.floor(expert * 0.5) * 12.0 + expert * 2.0 + rank
        spots = jnp.concatenate([spot + 4.0 * j for j in range(4)], axis=0)
        sel[k] = chosen(packed == spots)
    kta[96:128] = jnp.zeros((32, 384), BF)
    ktb[224:256] = jnp.zeros((32, 384), BF)
    heads = (
        (slice(0, 128), kta, 0, scale_one * LOG2E),
        (slice(128, 384), ktb, 1, scale_two * LOG2E),
    )

    def block(ref, first):
        rope = ref[0:32, 0:384]
        lat = ref[32:416, :]
        keys = lax.dot_general(
            wkt[...], lat, (((1,), (1,)), ((), ())), preferred_element_type=F32
        ).astype(BF)
        kta[0:64] = keys[0:64]
        kta[64:96] = rope
        ktb[0:192] = keys[64:256]
        ktb[192:224] = rope
        vx[...] = jnp.dot(lat, wv_ref[...], preferred_element_type=F32).astype(BF)
        for cols, keys_ref, h, factor in heads:
            scores = jnp.dot(qx[:, cols], keys_ref[...], preferred_element_type=F32)
            if first:
                rows = lax.broadcasted_iota(jnp.int32, (384, 384), 0)
                places = lax.broadcasted_iota(jnp.int32, (384, 384), 1)
                scores = jnp.where(rows >= places, scores, floor_score)
            peak = jnp.max(scores, axis=1, keepdims=True)
            width = (cols.stop - cols.start) // 128
            if first:
                new = jnp.broadcast_to(peak, (384, 128))
            else:
                old = top[h]
                new = jnp.maximum(old, peak)
            top[h] = new
            weights = jnp.exp2((scores - jnp.concatenate([new] * 3, axis=1)) * factor)
            sums = weights[:, 0:128] + weights[:, 128:256] + weights[:, 256:384]
            update = jnp.dot(weights.astype(BF), vx[:, 0 : 128 * width], preferred_element_type=F32)
            if first:
                weight_sum[h] = sums
                acc[:, cols] = update
            else:
                shrink = jnp.exp2((old - new) * factor)
                weight_sum[h] = weight_sum[h] * shrink + sums
                acc[:, cols] = acc[:, cols] * jnp.concatenate([shrink] * width, axis=1) + update

    for sign in (1, -1):
        send(None, slot(0, -sign), along_b(sign))
    block(own_ref, True)

    def step(i, carry):
        @pl.when(i == 1)
        def _():
            near = []
            for sign in (1, -1):
                k = slot(-sign, 0)
                arrived(k)
                flip(k)
                send(k, slot(-2 * sign, 0), along_a(sign), 0 if sign == 1 else 1)
                near.append(k)
                k = slot(0, -sign)
                arrived(k)
                flip(k)
                send(k, slot(0, -2 * sign), along_b(sign), 0 if sign == 1 else 1)
            for sign, k in zip((1, -1), near):
                send(k, slot(-sign, -1), along_b(1))
                send(k, slot(-sign, 1), along_b(-1))

        @pl.when(i == 3)
        def _():
            k = slot(2, 0)
            arrived(k, 0)
            arrived(k, 1)
            flip(k)
            send(k, slot(2, -1), along_b(1))
            send(k, slot(2, 1), along_b(-1))
            k = slot(0, 2)
            arrived(k, 0)
            arrived(k, 1)
            flip(k)

        @pl.when(i == 6)
        def _():
            for da in (-1, 1):
                for sign in (1, -1):
                    k = slot(da, -sign)
                    arrived(k)
                    flip(k)
                    send(k, slot(da, -2 * sign), along_b(sign), 0 if sign == 1 else 1)

        @pl.when(i == 7)
        def _():
            for sign in (1, -1):
                k = slot(2, -sign)
                arrived(k)
                flip(k)
                send(k, slot(2, -2 * sign), along_b(sign), 0 if sign == 1 else 1)

        @pl.when(i == 9)
        def _():
            for da in (-1, 1):
                k = slot(da, 2)
                arrived(k, 0)
                arrived(k, 1)
                flip(k)

        @pl.when(i == 10)
        def _():
            k = slot(2, 2)
            arrived(k, 0)
            arrived(k, 1)
            flip(k)

        flipped(i)
        dy = 0
        dx = 0
        for k in range(1, 16):
            dy = jnp.where(i == k, ORDER[k][0], dy)
            dx = jnp.where(i == k, ORDER[k][1], dx)
        theirs = ((y + dy) % 4) * 4 + (x + dx) % 4

        @pl.when(theirs < me)
        def _():
            block(buf.at[i - 1], False)

        return carry

    lax.fori_loop(1, 16, step, 0)

    total = acc[...]
    part_a = total[:, 0:128] / jnp.sum(weight_sum[0], axis=1, keepdims=True)
    part_b = total[:, 128:384] / jnp.sum(weight_sum[1], axis=1, keepdims=True)
    low = lax.broadcasted_iota(jnp.int32, (384, 128), 1) < DV_A
    both = jnp.concatenate([jnp.where(low, part_a, part_b[:, 0:128]), part_b[:, 128:256]], axis=1)
    for side in (0, 1):
        attx[side] = jnp.concatenate(
            [both[(2 * k + side) * 24 : (2 * k + side + 1) * 24] for k in range(8)], axis=0
        ).astype(BF)
    heads_over = pltpu.make_async_remote_copy(
        src_ref=attx.at[1 - c], dst_ref=attr, send_sem=misc_send.at[1], recv_sem=misc_recv.at[1],
        device_id=partner, device_id_type=MESH,
    )
    heads_over.start()
    weights_over.wait_recv()
    partial = jnp.dot(attx[c], ow_ref[...], preferred_element_type=F32)
    heads_over.wait_recv()
    partial = partial + jnp.dot(attr[...], owp[...], preferred_element_type=F32)
    part[...] = partial.reshape(8, 24, 2048)

    sent = []
    chains = {}

    def pass_on(way, side, hop, value):
        step_out[way, side, hop] = value.astype(BF)
        copy = pltpu.make_async_remote_copy(
            src_ref=step_out.at[way, side, hop], dst_ref=step_in.at[way, side, hop],
            send_sem=head_send.at[way, side, hop], recv_sem=head_recv.at[way, side, hop],
            device_id=along_z(1 if way == 0 else -1), device_id_type=MESH,
        )
        copy.start()
        sent.append(copy)
        chains[way, side] = copy

    def head_part(dz, side):
        return part[(z + dz + 8) % 8, :, side * 512 : (side + 1) * 512]

    far = ((0, 0), (1, 2), (0, 1), (1, 3))
    near = ((0, 2), (1, 0), (0, 3), (1, 1))
    for way, side in far:
        pass_on(way, side, 0, head_part(4, side))
    for way, side in near:
        pass_on(way, side, 1, head_part(3 if way == 0 else -3, side))
    for hop in (1, 2, 3):
        for way, side in far:
            chains[way, side].wait_recv()
            dz = (4 - hop) * (1 if way == 0 else -1)
            got = step_in[way, side, hop - 1].astype(F32)
            pass_on(way, side, hop, head_part(dz, side) + got)
        if hop < 3:
            for way, side in near:
                chains[way, side].wait_recv()
                dz = (3 - hop) * (1 if way == 0 else -1)
                got = step_in[way, side, hop].astype(F32)
                pass_on(way, side, hop + 1, head_part(dz, side) + got)
    for chain in chains.values():
        chain.wait_recv()
    arrived_sums = [
        jnp.concatenate([step_in[way, side, 3] for side in range(4)], axis=1).astype(F32)
        for way in (0, 1)
    ]
    mixed = residual_ref[...].astype(F32) + part[z]
    mixed = mixed + arrived_sums[0] + arrived_sums[1]
    mixed_ref[...] = mixed
    inverse = lax.rsqrt(jnp.mean(mixed * mixed, axis=1, keepdims=True) + epsilon)
    normed = mixed * inverse * gain_ref[...]
    stack = jnp.concatenate([normed[:, j * 512 : (j + 1) * 512] for j in range(4)], axis=0)
    outgoing = lax.dot_general(
        sel[0] + sel[1], stack.astype(BF), (((0,), (0,)), ((), ())), preferred_element_type=F32
    ).astype(BF)
    disp[...] = outgoing.reshape(16, 16, 512)

    def exchange(source, target, send_sem, recv_sem):
        target[me] = source[me]
        moves = []
        for dy, dx, peer in peers:
            there = peer[0] * 4 + peer[1]
            k = dy * 4 + dx - 1
            copy = pltpu.make_async_remote_copy(
                src_ref=source.at[there], dst_ref=target.at[me],
                send_sem=send_sem.at[k], recv_sem=recv_sem.at[k],
                device_id=peer, device_id_type=MESH,
            )
            copy.start()
            moves.append(copy)
        for copy in moves:
            copy.wait_recv()
        return moves

    moves = exchange(disp, arr, disp_send, disp_recv)
    order = lax.broadcasted_iota(jnp.int32, (256, 256), 0)
    order = ((order // 2) % 16) * 16 + (order // 64) * 4 + ((order // 32) % 2) * 2 + order % 2
    unpack = chosen(lax.broadcasted_iota(jnp.int32, (256, 256), 1) == order)
    arrived_rows = jnp.dot(
        unpack, arr[...].reshape(256, 512), preferred_element_type=F32
    ).astype(BF)
    for j in range(4):
        piece_rows = arrived_rows[j * 64 : (j + 1) * 64].reshape(2, 32, 512)
        rows_ref[:, :, j * 512 : (j + 1) * 512] = piece_rows

    copies = []

    def remote(src, dst, send_sem, recv_sem, device):
        copy = pltpu.make_async_remote_copy(
            src_ref=src, dst_ref=dst, send_sem=send_sem, recv_sem=recv_sem,
            device_id=device, device_id_type=MESH,
        )
        copy.start()
        copies.append(copy)
        return copy

    hops = {}
    swaps = {}
    ways = ((0, 1), (1, -1))

    def expert_of(way, unit):
        return unit if way == 0 else 1 - unit

    for unit in (0, 1):
        for way, sign in ways:
            e = expert_of(way, unit)
            hops[way, 1, e] = remote(
                rows_ref.at[e], held.at[e, BASE[-sign] + c],
                z_send.at[way, 0, e], z_recv.at[way, 0, e], along_z(sign),
            )
    for e in (0, 1):
        swaps[0, e] = remote(
            rows_ref.at[e], held.at[e, c], swap_send.at[0, e], swap_recv.at[0, e], partner
        )
        held[e, c] = rows_ref[e]

    def compute(e, dz):
        first = BASE[dz]
        k = first // 2
        swaps[k, e].wait_recv()
        rows = held[e, first : first + 2].reshape(64, 2048)
        inner = jnp.dot(rows, gate[e], preferred_element_type=F32)
        inner = inner / (1.0 + jnp.exp(-inner))
        inner = inner * jnp.dot(rows, up[e], preferred_element_type=F32)
        result = jnp.dot(inner.astype(BF), down[e], preferred_element_type=F32)
        made[e, first : first + 2] = result.astype(BF).reshape(2, 32, 2048)
        gives[dz, e] = remote(
            made.at[e, first + 1 - c], given.at[e, k], give_send.at[k, e], give_recv.at[k, e],
            partner,
        )

    def relay(dist, unit):
        for way, sign in ways:
            e = expert_of(way, unit)
            hops[way, dist, e].wait_recv()
            dz = -sign * dist
            spot = held.at[e, BASE[dz] + c]
            k = BASE[dz] // 2
            target = None
            if dist < 3:
                target = held.at[e, BASE[dz - sign] + c]
            elif unit == 0:
                target = held.at[e, BASE[4] + c]
            if target is not None:
                hops[way, dist + 1, e] = remote(
                    spot, target, z_send.at[way, dist, e], z_recv.at[way, dist, e], along_z(sign)
                )
            swaps[k, e] = remote(spot, spot, swap_send.at[k, e], swap_recv.at[k, e], partner)

    def work(dist, unit):
        for way, sign in ways:
            compute(expert_of(way, unit), -sign * dist)

    gives = {}

    def chip_sum(dz, e, side):
        if (dz, e) in gives:
            gives.pop((dz, e)).wait_recv()
        rows = slice(side * 16, (side + 1) * 16)
        mine = made[e, BASE[dz] + c, rows].astype(F32)
        return mine + given[e, BASE[dz] // 2, rows].astype(F32)

    for load in loads:
        load.wait()
    for e in (0, 1):
        compute(e, 0)
    relay(1, 0)
    relay(1, 1)
    work(1, 0)
    relay(2, 0)
    work(1, 1)
    relay(2, 1)
    work(2, 0)
    relay(3, 0)
    work(2, 1)
    work(3, 0)
    relay(3, 1)

    sums = {}

    def push(way, e, side, hop, value):
        rs_out[way, e, side, hop] = value.astype(BF)
        sums[way, e, side] = remote(
            rs_out.at[way, e, side, hop], rs_in.at[way, e, side, hop],
            rs_send.at[way, e, side, hop], rs_recv.at[way, e, side, hop],
            along_z(1 if way == 0 else -1),
        )

    def carry_on(way, e, dz, hop, sides=(0, 1)):
        for side in sides:
            sums[way, e, side].wait_recv()
            got = rs_in[way, e, side, hop - 1].astype(F32)
            push(way, e, side, hop, chip_sum(dz, e, side) + got)

    for way, e, dz in ((0, 1, 3), (1, 0, -3)):
        for side in (0, 1):
            push(way, e, side, 1, chip_sum(dz, e, side))
    work(3, 1)
    for e in (0, 1):
        hops[e, 4, e].wait_recv()
        spot = held.at[e, BASE[4] + c]
        swaps[7, e] = remote(spot, spot, swap_send.at[7, e], swap_recv.at[7, e], partner)
    for e in (0, 1):
        compute(e, 4)
    carry_on(0, 1, 2, 2, (0,))
    carry_on(1, 0, -2, 2, (0,))
    for way, e in ((0, 0), (1, 1)):
        for side in (0, 1):
            push(way, e, side, 0, chip_sum(4, e, side))
    carry_on(0, 1, 2, 2, (1,))
    carry_on(1, 0, -2, 2, (1,))
    carry_on(0, 0, 3, 1)
    carry_on(1, 1, -3, 1)
    carry_on(0, 1, 1, 3)
    carry_on(1, 0, -1, 3)
    carry_on(0, 0, 2, 2)
    carry_on(1, 1, -2, 2)
    carry_on(0, 0, 1, 3)
    carry_on(1, 1, -1, 3)
    for e in (0, 1):
        for side in (0, 1):
            own = chip_sum(0, e, side)
            for way in (0, 1):
                sums[way, e, side].wait_recv()
                own = own + rs_in[way, e, side, 3].astype(F32)
            sums_ref[e, side * 16 : (side + 1) * 16] = own.astype(BF)
    collected = jnp.concatenate(
        [sums_ref[:, :, j * 512 : (j + 1) * 512].reshape(64, 512) for j in range(4)], axis=0
    )
    order = lax.broadcasted_iota(jnp.int32, (256, 256), 1)
    order = ((order // 2) % 16) * 16 + (order // 64) * 4 + ((order // 32) % 2) * 2 + order % 2
    repack = chosen(lax.broadcasted_iota(jnp.int32, (256, 256), 0) == order)
    ret[...] = (
        jnp.dot(repack, collected, preferred_element_type=F32).astype(BF).reshape(16, 16, 512)
    )
    moves += exchange(ret, back, back_send, back_recv)
    returned = back[...].reshape(256, 512)
    result = mixed_ref[...]
    eye = lax.broadcasted_iota(jnp.int32, (24, 24), 0)
    eye = eye == lax.broadcasted_iota(jnp.int32, (24, 24), 1)
    groups = jnp.sum(jnp.where(eye, group_ref[...], 0.0), axis=1, keepdims=True)
    shares = [
        jnp.sum(jnp.where(eye, share_ref[k : k + 1], 0.0), axis=1, keepdims=True) for k in (0, 1)
    ]
    for k in (0, 1):
        picked = jnp.dot(sel[k], returned, preferred_element_type=F32)
        picked = jnp.concatenate([picked[j * 24 : (j + 1) * 24] for j in range(4)], axis=1)
        result = result + groups * shares[k] / (shares[0] + shares[1]) * picked
    out_ref[...] = result
    for copy in copies + moves:
        copy.wait_send()
    ends = [(ring_send.at[k], size) for k, size in ring]
    ends += [(flip_send.at[k], HALF) for k in range(15)]
    for sem, size in ends:
        pltpu.make_async_remote_copy(
            src_ref=buf.at[0, pl.ds(0, size)], dst_ref=buf.at[0, pl.ds(0, size)],
            send_sem=sem, recv_sem=flip_recv.at[0], device_id=partner, device_id_type=MESH,
        ).wait_send()
    for copy in sent + [weights_over, heads_over]:
        copy.wait_send()


def layer(operands, weights, scale_one, scale_two):
    vmem = pl.BlockSpec(memory_space=pltpu.VMEM)
    hbm = pl.BlockSpec(memory_space=pl.ANY)
    dma = pltpu.SemaphoreType.DMA
    return pl.pallas_call(
        functools.partial(layer_kernel, scale_one=scale_one, scale_two=scale_two),
        out_shape=jax.ShapeDtypeStruct((24, 2048), F32),
        in_specs=[vmem] * len(operands) + [hbm] * len(weights),
        out_specs=vmem,
        scratch_shapes=[
            pltpu.VMEM((416, 512), BF),
            pltpu.VMEM((2, 96, 256), BF),
            pltpu.VMEM((384, 384), BF),
            pltpu.VMEM((256, 512), BF),
            pltpu.VMEM((15, 416, 512), BF),
            pltpu.VMEM((128, 384), BF),
            pltpu.VMEM((256, 384), BF),
            pltpu.VMEM((384, 256), BF),
            pltpu.VMEM((384, 384), F32),
            pltpu.VMEM((2, 384, 128), F32),
            pltpu.VMEM((2, 384, 128), F32),
            pltpu.VMEM((256, 2048), BF),
            pltpu.VMEM((2, 192, 256), BF),
            pltpu.VMEM((192, 256), BF),
            pltpu.VMEM((8, 24, 2048), F32),
            pltpu.VMEM((2, 4, 4, 24, 512), BF),
            pltpu.VMEM((2, 4, 4, 24, 512), BF),
            pltpu.VMEM((24, 2048), F32),
            pltpu.VMEM((16, 16, 512), BF),
            pltpu.VMEM((16, 16, 512), BF),
            pltpu.VMEM((2, 32, 2048), BF),
            pltpu.VMEM((2, 16, 32, 2048), BF),
            pltpu.VMEM((2, 2048, 256), BF),
            pltpu.VMEM((2, 2048, 256), BF),
            pltpu.VMEM((2, 256, 2048), BF),
            pltpu.VMEM((2, 16, 32, 2048), BF),
            pltpu.VMEM((2, 8, 32, 2048), BF),
            pltpu.VMEM((2, 2, 2, 4, 16, 2048), BF),
            pltpu.VMEM((2, 2, 2, 4, 16, 2048), BF),
            pltpu.VMEM((2, 32, 2048), BF),
            pltpu.VMEM((16, 16, 512), BF),
            pltpu.VMEM((16, 16, 512), BF),
            dma((20,)),
            dma((15, 2)),
            dma((15,)),
            dma((15,)),
            dma((2,)),
            dma((2,)),
            dma((2, 4, 4)),
            dma((2, 4, 4)),
            dma((15,)),
            dma((15,)),
            dma((3,)),
            dma((2, 4, 2)),
            dma((2, 4, 2)),
            dma((8, 2)),
            dma((8, 2)),
            dma((8, 2)),
            dma((8, 2)),
            dma((2, 2, 2, 4)),
            dma((2, 2, 2, 4)),
            dma((15,)),
            dma((15,)),
        ],
        compiler_params=pltpu.CompilerParams(
            collective_id=0, has_side_effects=True, vmem_limit_bytes=60 * 1024 * 1024
        ),
        name="layer",
    )(*operands, *weights)


def local(
    residual,
    queries,
    query_rope,
    latent,
    key_rope,
    latent_gain,
    key_weight,
    value_weight,
    out_weight,
    norm_gain,
    routes,
    group_gate,
    expert_share,
    gate_weight,
    up_weight,
    down_weight,
):
    rope_width = key_rope.shape[1]
    scale_one = (DK_A + rope_width) ** (-0.5)
    scale_two = (queries.shape[2] - DK_A + rope_width) ** (-0.5)
    pace = np.float64(rope_base) ** (-np.arange(0, rope_width, 2) / rope_width)
    operands = (
        queries[:, 0],
        query_rope[:, 0].T,
        latent,
        key_rope.T,
        latent_gain[None],
        jnp.asarray(pace[:, None], F32),
        key_weight[:, 0],
        value_weight[:, 0],
        out_weight[0],
        residual,
        norm_gain[None],
        routes.T,
        group_gate[None],
        expert_share.T,
    )
    out = layer(operands, (gate_weight, up_weight, down_weight), scale_one, scale_two)
    return out.astype(BF)


def solution(mesh):
    finer = Mesh(mesh.devices.reshape(4, 4, 8, 2), ("y", "x", "z", "c"))
    placed = (
        P(SP_TP, None),
        P(SP, TP, None),
        P(SP, TP, None),
        P(SP, None),
        P(SP, None),
        P(),
        P(None, TP, None),
        P(None, TP, None),
        P(TP, None, None),
        P(),
        P(SP, None),
        P(SP_TP),
        P(SP_TP, None),
        P(SP, None, TP),
        P(SP, None, TP),
        P(SP, TP, None),
    )
    return jax.shard_map(
        local, mesh=finer, in_specs=placed, out_specs=P(SP_TP, None), check_vma=False
    )
```

```python
import functools

import jax
import jax.numpy as jnp
import numpy as np
from jax import lax
from jax.experimental import pallas as pl
from jax.experimental.pallas import tpu as pltpu
from jax.sharding import Mesh
from jax.sharding import PartitionSpec as P

DK_A = 64
DV_A = 64
SP = ("y", "x")
TP = ("z", "c")
SP_TP = ("y", "x", "z", "c")
MESH = pl.DeviceIdType.MESH
LOG2E = 1.4426950408889634
BF = jnp.bfloat16
F32 = jnp.float32

rope_base = 10000.0
epsilon = 1e-06
floor_score = -1e30

ORDER = (
    (0, 0),
    (0, 1), (0, 3), (1, 0), (3, 0),
    (0, 2), (2, 0),
    (1, 1), (1, 3), (3, 1), (3, 3),
    (1, 2), (3, 2), (2, 1), (2, 3),
    (2, 2),
)
SLOT = {place: k for k, place in enumerate(ORDER)}
HALF = 208
PART = 112


def place():
    return tuple(lax.axis_index(name) for name in ("y", "x", "z", "c"))


def meet(devices):
    barrier = pltpu.get_barrier_semaphore()
    for device in devices:
        pl.semaphore_signal(barrier, inc=1, device_id=device, device_id_type=MESH)
    pl.semaphore_wait(barrier, len(devices))


DZ = (0, -1, 1, -2, 2, -3, 3, 4)
BASE = {dz: 2 * k for k, dz in enumerate(DZ)}


def spread_place(column):
    return column + jnp.where(column >= DK_A, 64, 0)


def chosen(condition):
    return jnp.where(condition, 1.0, 0.0).astype(BF)


def layer_kernel(
    q_ref, q_rope_ref, latent_ref, key_rope_ref, latent_gain_ref, pace_ref,
    wk_ref, wv_ref, ow_ref, residual_ref, gain_ref,
    routes_ref, group_ref, share_ref, gate_hbm, up_hbm, down_hbm, out_ref,
    own_ref, sel, qx, wkt, buf, kta, ktb, vx, acc, top, weight_sum, owp, attx, attr, part,
    step_out, step_in, mixed_ref, disp, arr, rows_ref,
    held, gate, up, down, made, given, rs_out, rs_in, sums_ref, ret, back,
    ring_send, ring_recv, flip_send, flip_recv, misc_send, misc_recv, head_send, head_recv,
    disp_send, disp_recv, load_sem, z_send, z_recv, swap_send, swap_recv,
    give_send, give_recv, rs_send, rs_recv, back_send, back_recv,
    *, scale_one, scale_two,
):
    y, x, z, c = place()
    partner = (y, x, z, 1 - c)

    def along_a(step):
        return ((y + c * step + 4) % 4, (x + (1 - c) * step + 4) % 4, z, c)

    def along_b(step):
        return ((y + (1 - c) * step + 4) % 4, (x + c * step + 4) % 4, z, c)

    def along_z(step):
        return (y, x, (z + step + 8) % 8, c)

    def slot(da, db):
        first = SLOT[(db % 4, da % 4)]
        second = SLOT[(da % 4, db % 4)]
        return first if first == second else first + c * (second - first)

    me = y * 4 + x
    peers = [
        (dy, dx, ((y + dy) % 4, (x + dx) % 4, z, c))
        for dy, dx in sorted(ORDER[1:], key=lambda p: -(min(p[0], 4 - p[0]) + min(p[1], 4 - p[1])))
    ]
    loads = [
        pltpu.make_async_copy(src, dst, load_sem.at[k])
        for k, (src, dst) in enumerate(((gate_hbm, gate), (up_hbm, up), (down_hbm, down)))
    ]
    for load in loads:
        load.start()
    angles = (me * 384 + lax.broadcasted_iota(jnp.int32, (16, 384), 1)).astype(F32)
    angles = angles * pace_ref[...]
    cosine = jnp.cos(angles)
    sine = jnp.sin(angles)

    def turn(pair):
        first, second = pair[0:16], pair[16:32]
        return [first * cosine - second * sine, second * cosine + first * sine]

    keys = key_rope_ref[...].astype(F32)
    own_ref[0:32, 0:384] = jnp.concatenate(turn(keys), axis=0).astype(BF)
    own_ref[0:32, 384:512] = jnp.zeros((32, 128), BF)
    latent = latent_ref[...].astype(F32)
    inverse = lax.rsqrt(jnp.mean(latent * latent, axis=1, keepdims=True) + epsilon)
    own_ref[32:416] = (latent * inverse * latent_gain_ref[...]).astype(BF)
    meet([partner, along_z(1), along_z(-1)] + [peer[2] for peer in peers])
    start_row = c * HALF
    other_row = (1 - c) * HALF
    counts = {"ring": 0}
    ring = []

    def piece(k, first, size):
        return buf.at[k - 1, pl.ds(pl.multiple_of(start_row + first, 16), size)]

    spans = {None: (0, HALF), 0: (0, PART), 1: (PART, HALF - PART)}

    def send(source, target, device, which=None):
        first, size = spans[which]
        if source is None:
            src = own_ref.at[pl.ds(pl.multiple_of(start_row + first, 16), size)]
        else:
            src = piece(source, first, size)
        copy = pltpu.make_async_remote_copy(
            src_ref=src,
            dst_ref=piece(target, first, size),
            send_sem=ring_send.at[counts["ring"]],
            recv_sem=ring_recv.at[target - 1, which or 0],
            device_id=device,
            device_id_type=MESH,
        )
        ring.append((counts["ring"], size))
        counts["ring"] += 1
        copy.start()

    def arrived(k, which=None):
        first, size = spans[which]
        pltpu.make_async_remote_copy(
            src_ref=piece(k, first, size),
            dst_ref=piece(k, first, size),
            send_sem=ring_send.at[0],
            recv_sem=ring_recv.at[k - 1, which or 0],
            device_id=partner,
            device_id_type=MESH,
        ).wait_recv()

    def flip(k):
        copy = pltpu.make_async_remote_copy(
            src_ref=piece(k, 0, HALF),
            dst_ref=piece(k, 0, HALF),
            send_sem=flip_send.at[k - 1],
            recv_sem=flip_recv.at[k - 1],
            device_id=partner,
            device_id_type=MESH,
        )
        copy.start()

    def flipped(k):
        there = buf.at[k - 1, pl.ds(pl.multiple_of(other_row, 16), HALF)]
        pltpu.make_async_remote_copy(
            src_ref=there, dst_ref=there,
            send_sem=flip_send.at[0], recv_sem=flip_recv.at[k - 1],
            device_id=partner, device_id_type=MESH,
        ).wait_recv()

    for sign in (1, -1):
        send(None, slot(-sign, 0), along_a(sign))
    weights_over = pltpu.make_async_remote_copy(
        src_ref=ow_ref, dst_ref=owp, send_sem=misc_send.at[0], recv_sem=misc_recv.at[0],
        device_id=partner, device_id_type=MESH,
    )
    weights_over.start()

    queries = q_rope_ref[...].astype(F32)
    turned = jnp.concatenate(turn(queries[0:32]) + turn(queries[32:64]), axis=0).astype(BF)
    spread = chosen(
        lax.broadcasted_iota(jnp.int32, (256, 384), 1)
        == spread_place(lax.broadcasted_iota(jnp.int32, (256, 384), 0))
    )
    turns = lax.broadcasted_iota(jnp.int32, (64, 384), 0)
    turns = chosen(
        lax.broadcasted_iota(jnp.int32, (64, 384), 1)
        == turns + 64 + jnp.where(turns >= 32, 224, 0)
    )
    qx[...] = (
        jnp.dot(q_ref[...], spread, preferred_element_type=F32)
        + lax.dot_general(
            turned, turns, (((0,), (0,)), ((), ())), preferred_element_type=F32
        )
    ).astype(BF)
    unit = chosen(
        lax.broadcasted_iota(jnp.int32, (256, 256), 0)
        == lax.broadcasted_iota(jnp.int32, (256, 256), 1)
    )
    wkt[...] = lax.dot_general(
        unit, wk_ref[...], (((1,), (1,)), ((), ())), preferred_element_type=F32
    ).astype(BF)
    tokens = lax.broadcasted_iota(jnp.int32, (24, 384), 0) + (z * 2 + c) * 24
    mine = chosen(lax.broadcasted_iota(jnp.int32, (24, 384), 1) == tokens)
    routes = lax.dot_general(
        mine, routes_ref[...].astype(F32).astype(BF), (((1,), (1,)), ((), ())),
        preferred_element_type=F32,
    )
    experts = lax.broadcasted_iota(jnp.int32, (24, 32), 1).astype(F32)
    named = [routes[:, k : k + 1] == experts for k in (0, 1)]
    earlier = chosen(
        lax.broadcasted_iota(jnp.int32, (24, 24), 0) > lax.broadcasted_iota(jnp.int32, (24, 24), 1)
    )
    before = jnp.dot(earlier, chosen(named[0] | named[1]), preferred_element_type=F32)
    packed = lax.broadcasted_iota(jnp.int32, (96, 256), 1).astype(F32)
    for k in (0, 1):
        rank = jnp.sum(jnp.where(named[k], before, 0.0), axis=1, keepdims=True)
        expert = routes[:, k : k + 1]
        spot = jnp.floor(expert * 0.5) * 12.0 + expert * 2.0 + rank
        spots = jnp.concatenate([spot + 4.0 * j for j in range(4)], axis=0)
        sel[k] = chosen(packed == spots)
    kta[96:128] = jnp.zeros((32, 384), BF)
    ktb[224:256] = jnp.zeros((32, 384), BF)
    heads = (
        (slice(0, 128), kta, 0, scale_one * LOG2E),
        (slice(128, 384), ktb, 1, scale_two * LOG2E),
    )

    def block(ref, first):
        rope = ref[0:32, 0:384]
        lat = ref[32:416, :]
        keys = lax.dot_general(
            wkt[...], lat, (((1,), (1,)), ((), ())), preferred_element_type=F32
        ).astype(BF)
        kta[0:64] = keys[0:64]
        kta[64:96] = rope
        ktb[0:192] = keys[64:256]
        ktb[192:224] = rope
        vx[...] = jnp.dot(lat, wv_ref[...], preferred_element_type=F32).astype(BF)
        products = [
            jnp.dot(qx[:, cols], keys_ref[...], preferred_element_type=F32)
            for cols, keys_ref, h, factor in heads
        ]
        for (cols, keys_ref, h, factor), scores in zip(heads, products):
            if first:
                rows = lax.broadcasted_iota(jnp.int32, (384, 384), 0)
                places = lax.broadcasted_iota(jnp.int32, (384, 384), 1)
                scores = jnp.where(rows >= places, scores, floor_score)
            peak = jnp.max(scores, axis=1, keepdims=True)
            width = (cols.stop - cols.start) // 128
            if first:
                new = jnp.broadcast_to(peak, (384, 128))
            else:
                old = top[h]
                new = jnp.maximum(old, peak)
            top[h] = new
            weights = jnp.exp2((scores - jnp.concatenate([new] * 3, axis=1)) * factor)
            sums = weights[:, 0:128] + weights[:, 128:256] + weights[:, 256:384]
            update = jnp.dot(weights.astype(BF), vx[:, 0 : 128 * width], preferred_element_type=F32)
            if first:
                weight_sum[h] = sums
                acc[:, cols] = update
            else:
                shrink = jnp.exp2((old - new) * factor)
                weight_sum[h] = weight_sum[h] * shrink + sums
                acc[:, cols] = acc[:, cols] * jnp.concatenate([shrink] * width, axis=1) + update

    for sign in (1, -1):
        send(None, slot(0, -sign), along_b(sign))
    block(own_ref, True)

    def step(i, carry):
        @pl.when(i == 1)
        def _():
            near = []
            for sign in (1, -1):
                k = slot(-sign, 0)
                arrived(k)
                flip(k)
                send(k, slot(-2 * sign, 0), along_a(sign), 0 if sign == 1 else 1)
                near.append(k)
                k = slot(0, -sign)
                arrived(k)
                flip(k)
                send(k, slot(0, -2 * sign), along_b(sign), 0 if sign == 1 else 1)
            for sign, k in zip((1, -1), near):
                send(k, slot(-sign, -1), along_b(1))
                send(k, slot(-sign, 1), along_b(-1))

        @pl.when(i == 3)
        def _():
            k = slot(2, 0)
            arrived(k, 0)
            arrived(k, 1)
            flip(k)
            send(k, slot(2, -1), along_b(1))
            send(k, slot(2, 1), along_b(-1))
            k = slot(0, 2)
            arrived(k, 0)
            arrived(k, 1)
            flip(k)

        @pl.when(i == 6)
        def _():
            for da in (-1, 1):
                for sign in (1, -1):
                    k = slot(da, -sign)
                    arrived(k)
                    flip(k)
                    send(k, slot(da, -2 * sign), along_b(sign), 0 if sign == 1 else 1)

        @pl.when(i == 7)
        def _():
            for sign in (1, -1):
                k = slot(2, -sign)
                arrived(k)
                flip(k)
                send(k, slot(2, -2 * sign), along_b(sign), 0 if sign == 1 else 1)

        @pl.when(i == 9)
        def _():
            for da in (-1, 1):
                k = slot(da, 2)
                arrived(k, 0)
                arrived(k, 1)
                flip(k)

        @pl.when(i == 10)
        def _():
            k = slot(2, 2)
            arrived(k, 0)
            arrived(k, 1)
            flip(k)

        flipped(i)
        dy = 0
        dx = 0
        for k in range(1, 16):
            dy = jnp.where(i == k, ORDER[k][0], dy)
            dx = jnp.where(i == k, ORDER[k][1], dx)
        theirs = ((y + dy) % 4) * 4 + (x + dx) % 4

        @pl.when(theirs < me)
        def _():
            block(buf.at[i - 1], False)

        return carry

    lax.fori_loop(1, 16, step, 0)

    total = acc[...]
    part_a = total[:, 0:128] / jnp.sum(weight_sum[0], axis=1, keepdims=True)
    part_b = total[:, 128:384] / jnp.sum(weight_sum[1], axis=1, keepdims=True)
    low = lax.broadcasted_iota(jnp.int32, (384, 128), 1) < DV_A
    both = jnp.concatenate([jnp.where(low, part_a, part_b[:, 0:128]), part_b[:, 128:256]], axis=1)
    for side in (0, 1):
        attx[side] = jnp.concatenate(
            [both[(2 * k + side) * 24 : (2 * k + side + 1) * 24] for k in range(8)], axis=0
        ).astype(BF)
    heads_over = pltpu.make_async_remote_copy(
        src_ref=attx.at[1 - c], dst_ref=attr, send_sem=misc_send.at[1], recv_sem=misc_recv.at[1],
        device_id=partner, device_id_type=MESH,
    )
    heads_over.start()
    weights_over.wait_recv()
    partial = jnp.dot(attx[c], ow_ref[...], preferred_element_type=F32)
    heads_over.wait_recv()
    partial = partial + jnp.dot(attr[...], owp[...], preferred_element_type=F32)
    part[...] = partial.reshape(8, 24, 2048)

    sent = []
    chains = {}

    def pass_on(way, side, hop, value):
        step_out[way, side, hop] = value.astype(BF)
        copy = pltpu.make_async_remote_copy(
            src_ref=step_out.at[way, side, hop], dst_ref=step_in.at[way, side, hop],
            send_sem=head_send.at[way, side, hop], recv_sem=head_recv.at[way, side, hop],
            device_id=along_z(1 if way == 0 else -1), device_id_type=MESH,
        )
        copy.start()
        sent.append(copy)
        chains[way, side] = copy

    def head_part(dz, side):
        return part[(z + dz + 8) % 8, :, side * 512 : (side + 1) * 512]

    far = ((0, 0), (1, 2), (0, 1), (1, 3))
    near = ((0, 2), (1, 0), (0, 3), (1, 1))
    for way, side in far:
        pass_on(way, side, 0, head_part(4, side))
    for way, side in near:
        pass_on(way, side, 1, head_part(3 if way == 0 else -3, side))
    for hop in (1, 2, 3):
        for way, side in far:
            chains[way, side].wait_recv()
            dz = (4 - hop) * (1 if way == 0 else -1)
            got = step_in[way, side, hop - 1].astype(F32)
            pass_on(way, side, hop, head_part(dz, side) + got)
        if hop < 3:
            for way, side in near:
                chains[way, side].wait_recv()
                dz = (3 - hop) * (1 if way == 0 else -1)
                got = step_in[way, side, hop].astype(F32)
                pass_on(way, side, hop + 1, head_part(dz, side) + got)
    for chain in chains.values():
        chain.wait_recv()
    arrived_sums = [
        jnp.concatenate([step_in[way, side, 3] for side in range(4)], axis=1).astype(F32)
        for way in (0, 1)
    ]
    mixed = residual_ref[...].astype(F32) + part[z]
    mixed = mixed + arrived_sums[0] + arrived_sums[1]
    mixed_ref[...] = mixed
    inverse = lax.rsqrt(jnp.mean(mixed * mixed, axis=1, keepdims=True) + epsilon)
    normed = mixed * inverse * gain_ref[...]
    stack = jnp.concatenate([normed[:, j * 512 : (j + 1) * 512] for j in range(4)], axis=0)
    outgoing = lax.dot_general(
        sel[0] + sel[1], stack.astype(BF), (((0,), (0,)), ((), ())), preferred_element_type=F32
    ).astype(BF)
    disp[...] = outgoing.reshape(16, 16, 512)

    def exchange(source, target, send_sem, recv_sem):
        target[me] = source[me]
        moves = []
        for dy, dx, peer in peers:
            there = peer[0] * 4 + peer[1]
            k = dy * 4 + dx - 1
            copy = pltpu.make_async_remote_copy(
                src_ref=source.at[there], dst_ref=target.at[me],
                send_sem=send_sem.at[k], recv_sem=recv_sem.at[k],
                device_id=peer, device_id_type=MESH,
            )
            copy.start()
            moves.append(copy)
        for copy in moves:
            copy.wait_recv()
        return moves

    moves = exchange(disp, arr, disp_send, disp_recv)
    order = lax.broadcasted_iota(jnp.int32, (256, 256), 0)
    order = ((order // 2) % 16) * 16 + (order // 64) * 4 + ((order // 32) % 2) * 2 + order % 2
    unpack = chosen(lax.broadcasted_iota(jnp.int32, (256, 256), 1) == order)
    arrived_rows = jnp.dot(
        unpack, arr[...].reshape(256, 512), preferred_element_type=F32
    ).astype(BF)
    for j in range(4):
        piece_rows = arrived_rows[j * 64 : (j + 1) * 64].reshape(2, 32, 512)
        rows_ref[:, :, j * 512 : (j + 1) * 512] = piece_rows

    copies = []

    def remote(src, dst, send_sem, recv_sem, device):
        copy = pltpu.make_async_remote_copy(
            src_ref=src, dst_ref=dst, send_sem=send_sem, recv_sem=recv_sem,
            device_id=device, device_id_type=MESH,
        )
        copy.start()
        copies.append(copy)
        return copy

    hops = {}
    swaps = {}
    ways = ((0, 1), (1, -1))

    def expert_of(way, unit):
        return unit if way == 0 else 1 - unit

    for unit in (0, 1):
        for way, sign in ways:
            e = expert_of(way, unit)
            hops[way, 1, e] = remote(
                rows_ref.at[e], held.at[e, BASE[-sign] + c],
                z_send.at[way, 0, e], z_recv.at[way, 0, e], along_z(sign),
            )
    for e in (0, 1):
        swaps[0, e] = remote(
            rows_ref.at[e], held.at[e, c], swap_send.at[0, e], swap_recv.at[0, e], partner
        )
        held[e, c] = rows_ref[e]

    def compute(e, dz):
        first = BASE[dz]
        k = first // 2
        swaps[k, e].wait_recv()
        rows = held[e, first : first + 2].reshape(64, 2048)
        inner = jnp.dot(rows, gate[e], preferred_element_type=F32)
        inner = inner / (1.0 + jnp.exp(-inner))
        inner = inner * jnp.dot(rows, up[e], preferred_element_type=F32)
        result = jnp.dot(inner.astype(BF), down[e], preferred_element_type=F32)
        made[e, first : first + 2] = result.astype(BF).reshape(2, 32, 2048)
        gives[dz, e] = remote(
            made.at[e, first + 1 - c], given.at[e, k], give_send.at[k, e], give_recv.at[k, e],
            partner,
        )

    def relay(dist, unit):
        for way, sign in ways:
            e = expert_of(way, unit)
            hops[way, dist, e].wait_recv()
            dz = -sign * dist
            spot = held.at[e, BASE[dz] + c]
            k = BASE[dz] // 2
            target = None
            if dist < 3:
                target = held.at[e, BASE[dz - sign] + c]
            elif unit == 0:
                target = held.at[e, BASE[4] + c]
            if target is not None:
                hops[way, dist + 1, e] = remote(
                    spot, target, z_send.at[way, dist, e], z_recv.at[way, dist, e], along_z(sign)
                )
            swaps[k, e] = remote(spot, spot, swap_send.at[k, e], swap_recv.at[k, e], partner)

    def work(dist, unit):
        for way, sign in ways:
            compute(expert_of(way, unit), -sign * dist)

    gives = {}

    def chip_sum(dz, e, side):
        if (dz, e) in gives:
            gives.pop((dz, e)).wait_recv()
        rows = slice(side * 16, (side + 1) * 16)
        mine = made[e, BASE[dz] + c, rows].astype(F32)
        return mine + given[e, BASE[dz] // 2, rows].astype(F32)

    for load in loads:
        load.wait()
    for e in (0, 1):
        compute(e, 0)
    relay(1, 0)
    relay(1, 1)
    work(1, 0)
    relay(2, 0)
    work(1, 1)
    relay(2, 1)
    work(2, 0)
    relay(3, 0)
    work(2, 1)
    work(3, 0)
    relay(3, 1)

    sums = {}

    def push(way, e, side, hop, value):
        rs_out[way, e, side, hop] = value.astype(BF)
        sums[way, e, side] = remote(
            rs_out.at[way, e, side, hop], rs_in.at[way, e, side, hop],
            rs_send.at[way, e, side, hop], rs_recv.at[way, e, side, hop],
            along_z(1 if way == 0 else -1),
        )

    def carry_on(way, e, dz, hop, sides=(0, 1)):
        for side in sides:
            sums[way, e, side].wait_recv()
            got = rs_in[way, e, side, hop - 1].astype(F32)
            push(way, e, side, hop, chip_sum(dz, e, side) + got)

    for way, e, dz in ((0, 1, 3), (1, 0, -3)):
        for side in (0, 1):
            push(way, e, side, 1, chip_sum(dz, e, side))
    work(3, 1)
    for e in (0, 1):
        hops[e, 4, e].wait_recv()
        spot = held.at[e, BASE[4] + c]
        swaps[7, e] = remote(spot, spot, swap_send.at[7, e], swap_recv.at[7, e], partner)
    for e in (0, 1):
        compute(e, 4)
    carry_on(0, 1, 2, 2, (0,))
    carry_on(1, 0, -2, 2, (0,))
    for way, e in ((0, 0), (1, 1)):
        for side in (0, 1):
            push(way, e, side, 0, chip_sum(4, e, side))
    carry_on(0, 1, 2, 2, (1,))
    carry_on(1, 0, -2, 2, (1,))
    carry_on(0, 0, 3, 1)
    carry_on(1, 1, -3, 1)
    carry_on(0, 1, 1, 3)
    carry_on(1, 0, -1, 3)
    carry_on(0, 0, 2, 2)
    carry_on(1, 1, -2, 2)
    carry_on(0, 0, 1, 3)
    carry_on(1, 1, -1, 3)
    for e in (0, 1):
        for side in (0, 1):
            own = chip_sum(0, e, side)
            for way in (0, 1):
                sums[way, e, side].wait_recv()
                own = own + rs_in[way, e, side, 3].astype(F32)
            sums_ref[e, side * 16 : (side + 1) * 16] = own.astype(BF)
    collected = jnp.concatenate(
        [sums_ref[:, :, j * 512 : (j + 1) * 512].reshape(64, 512) for j in range(4)], axis=0
    )
    order = lax.broadcasted_iota(jnp.int32, (256, 256), 1)
    order = ((order // 2) % 16) * 16 + (order // 64) * 4 + ((order // 32) % 2) * 2 + order % 2
    repack = chosen(lax.broadcasted_iota(jnp.int32, (256, 256), 0) == order)
    ret[...] = (
        jnp.dot(repack, collected, preferred_element_type=F32).astype(BF).reshape(16, 16, 512)
    )
    moves += exchange(ret, back, back_send, back_recv)
    returned = back[...].reshape(256, 512)
    result = mixed_ref[...]
    eye = lax.broadcasted_iota(jnp.int32, (24, 24), 0)
    eye = eye == lax.broadcasted_iota(jnp.int32, (24, 24), 1)
    groups = jnp.sum(jnp.where(eye, group_ref[...], 0.0), axis=1, keepdims=True)
    shares = [
        jnp.sum(jnp.where(eye, share_ref[k : k + 1], 0.0), axis=1, keepdims=True) for k in (0, 1)
    ]
    for k in (0, 1):
        picked = jnp.dot(sel[k], returned, preferred_element_type=F32)
        picked = jnp.concatenate([picked[j * 24 : (j + 1) * 24] for j in range(4)], axis=1)
        result = result + groups * shares[k] / (shares[0] + shares[1]) * picked
    out_ref[...] = result
    for copy in copies + moves:
        copy.wait_send()
    ends = [(ring_send.at[k], size) for k, size in ring]
    ends += [(flip_send.at[k], HALF) for k in range(15)]
    for sem, size in ends:
        pltpu.make_async_remote_copy(
            src_ref=buf.at[0, pl.ds(0, size)], dst_ref=buf.at[0, pl.ds(0, size)],
            send_sem=sem, recv_sem=flip_recv.at[0], device_id=partner, device_id_type=MESH,
        ).wait_send()
    for copy in sent + [weights_over, heads_over]:
        copy.wait_send()


def layer(operands, weights, scale_one, scale_two):
    vmem = pl.BlockSpec(memory_space=pltpu.VMEM)
    hbm = pl.BlockSpec(memory_space=pl.ANY)
    dma = pltpu.SemaphoreType.DMA
    return pl.pallas_call(
        functools.partial(layer_kernel, scale_one=scale_one, scale_two=scale_two),
        out_shape=jax.ShapeDtypeStruct((24, 2048), F32),
        in_specs=[vmem] * len(operands) + [hbm] * len(weights),
        out_specs=vmem,
        scratch_shapes=[
            pltpu.VMEM((416, 512), BF),
            pltpu.VMEM((2, 96, 256), BF),
            pltpu.VMEM((384, 384), BF),
            pltpu.VMEM((256, 512), BF),
            pltpu.VMEM((15, 416, 512), BF),
            pltpu.VMEM((128, 384), BF),
            pltpu.VMEM((256, 384), BF),
            pltpu.VMEM((384, 256), BF),
            pltpu.VMEM((384, 384), F32),
            pltpu.VMEM((2, 384, 128), F32),
            pltpu.VMEM((2, 384, 128), F32),
            pltpu.VMEM((256, 2048), BF),
            pltpu.VMEM((2, 192, 256), BF),
            pltpu.VMEM((192, 256), BF),
            pltpu.VMEM((8, 24, 2048), F32),
            pltpu.VMEM((2, 4, 4, 24, 512), BF),
            pltpu.VMEM((2, 4, 4, 24, 512), BF),
            pltpu.VMEM((24, 2048), F32),
            pltpu.VMEM((16, 16, 512), BF),
            pltpu.VMEM((16, 16, 512), BF),
            pltpu.VMEM((2, 32, 2048), BF),
            pltpu.VMEM((2, 16, 32, 2048), BF),
            pltpu.VMEM((2, 2048, 256), BF),
            pltpu.VMEM((2, 2048, 256), BF),
            pltpu.VMEM((2, 256, 2048), BF),
            pltpu.VMEM((2, 16, 32, 2048), BF),
            pltpu.VMEM((2, 8, 32, 2048), BF),
            pltpu.VMEM((2, 2, 2, 4, 16, 2048), BF),
            pltpu.VMEM((2, 2, 2, 4, 16, 2048), BF),
            pltpu.VMEM((2, 32, 2048), BF),
            pltpu.VMEM((16, 16, 512), BF),
            pltpu.VMEM((16, 16, 512), BF),
            dma((20,)),
            dma((15, 2)),
            dma((15,)),
            dma((15,)),
            dma((2,)),
            dma((2,)),
            dma((2, 4, 4)),
            dma((2, 4, 4)),
            dma((15,)),
            dma((15,)),
            dma((3,)),
            dma((2, 4, 2)),
            dma((2, 4, 2)),
            dma((8, 2)),
            dma((8, 2)),
            dma((8, 2)),
            dma((8, 2)),
            dma((2, 2, 2, 4)),
            dma((2, 2, 2, 4)),
            dma((15,)),
            dma((15,)),
        ],
        compiler_params=pltpu.CompilerParams(
            collective_id=0, has_side_effects=True, vmem_limit_bytes=60 * 1024 * 1024
        ),
        name="layer",
    )(*operands, *weights)


def local(
    residual,
    queries,
    query_rope,
    latent,
    key_rope,
    latent_gain,
    key_weight,
    value_weight,
    out_weight,
    norm_gain,
    routes,
    group_gate,
    expert_share,
    gate_weight,
    up_weight,
    down_weight,
):
    rope_width = key_rope.shape[1]
    scale_one = (DK_A + rope_width) ** (-0.5)
    scale_two = (queries.shape[2] - DK_A + rope_width) ** (-0.5)
    pace = np.float64(rope_base) ** (-np.arange(0, rope_width, 2) / rope_width)
    operands = (
        queries[:, 0],
        query_rope[:, 0].T,
        latent,
        key_rope.T,
        latent_gain[None],
        jnp.asarray(pace[:, None], F32),
        key_weight[:, 0],
        value_weight[:, 0],
        out_weight[0],
        residual,
        norm_gain[None],
        routes.T,
        group_gate[None],
        expert_share.T,
    )
    out = layer(operands, (gate_weight, up_weight, down_weight), scale_one, scale_two)
    return out.astype(BF)


def solution(mesh):
    finer = Mesh(mesh.devices.reshape(4, 4, 8, 2), ("y", "x", "z", "c"))
    placed = (
        P(SP_TP, None),
        P(SP, TP, None),
        P(SP, TP, None),
        P(SP, None),
        P(SP, None),
        P(),
        P(None, TP, None),
        P(None, TP, None),
        P(TP, None, None),
        P(),
        P(SP, None),
        P(SP_TP),
        P(SP_TP, None),
        P(SP, None, TP),
        P(SP, None, TP),
        P(SP, TP, None),
    )
    return jax.shard_map(
        local, mesh=finer, in_specs=placed, out_specs=P(SP_TP, None), check_vma=False
    )
```
